32 devices in a mesh: sp: 8 (over z, y), tp: 4 (over x, core).
Axes of the slice: x: 2, y: 2, z: 4, core: 2. Of those that a mesh axis runs over, the one named last changes fastest.
Arguments:
- tokens: bfloat16 [1280, 2048], P('sp'), may hold values from -6 to 6
- input_gain: float32 [2048], replicated, may hold values from 0.1 to 1.9
- chain_query: bfloat16 [2048, 1024], P('sp', 'tp'), may hold values from -0.125 to 0.125
- forward_gate: bfloat16 [2048, 1024], P('sp', 'tp'), may hold values from -0.125 to 0.125
- backward_gate: bfloat16 [2048, 1024], P('sp', 'tp'), may hold values from -0.125 to 0.125
- chain_value: bfloat16 [2048, 1024], P('sp', 'tp'), may hold values from -0.125 to 0.125
- output_gate: bfloat16 [2048, 1024], P('sp', 'tp'), may hold values from -0.125 to 0.125
- forget_rate: float32 [2, 1024], P(None, 'tp'), may hold values from 0.2 to 6
- chain_gain: float32 [1024], P('tp'), may hold values from 0.1 to 1.9
- query_down: bfloat16 [2048, 768], P('sp'), may hold values from -0.125 to 0.125
- latent_down: bfloat16 [2048, 512], P('sp'), may hold values from -0.125 to 0.125
- rotary_down: bfloat16 [2048, 64], replicated, may hold values from -0.125 to 0.125
- query_latent_gain: float32 [768], replicated, may hold values from 0.1 to 1.9
- latent_gain: float32 [512], replicated, may hold values from 0.1 to 1.9
- query_up: bfloat16 [768, 1536], P(None, 'tp'), may hold values from -0.21875 to 0.21875
- latent_up: bfloat16 [512, 2048], P(None, 'tp'), may hold values from -0.25 to 0.25
- query_head_gain: float32 [192], replicated, may hold values from 0.1 to 1.9
- key_head_gain: float32 [192], replicated, may hold values from 0.1 to 1.9
- mixer_gain: float32 [1024], P('tp'), may hold values from 0.1 to 1.9
- chain_out: bfloat16 [1024, 2048], P('tp', 'sp'), may hold values from -0.125 to 0.125
- attend_out: bfloat16 [1024, 2048], P('tp', 'sp'), may hold values from -0.125 to 0.125
Outputs:
- mixed: float32 [1280, 2048], P(('sp', 'tp'))
The draws below stay inside these ranges and needn't reach their ends.
All inputs are finite; a program needn't handle non-finite values.
Results may differ from the reference program's by a relative error of at most 0.017.
Values may be sent and summed in bfloat16 or wider, within the bound.
A program may use at most 128 MiB of HBM per device.

```python
import math
import jax
import jax.numpy as jnp
from jax import lax

D = 2048
KEY_DIM = 128
VAL_DIM = 128
HEADS_ATT = 8
NOPE_DIM = 128
ROPE_DIM = 64
VHEAD_DIM = 128
QLAT = 768
KVLAT = 512
TOK_DEV = 160
SEQ = 1280
REC_KEYS = 1024
REC_WIDTH = 1024
ATT_QK = 192
ATT_WIDTH = 1024


def block_levels(key, shape, cuts, low, top_value):
    factor_of = 1.0
    for dim, parts in cuts:
        draws = jax.random.uniform(jax.random.fold_in(jax.random.fold_in(key, 6), dim), (parts,), jnp.float32, low / len(cuts), top_value / len(cuts))
        factor_of = factor_of * jnp.repeat(jnp.exp(draws), shape[dim] // parts).reshape((-1,) + (1,) * (len(shape) - 1 - dim))
    return factor_of


def normal_values(stream_key, extent, width, bound, cuts=(), held_as=jnp.bfloat16):
    loudness = block_levels(stream_key, extent, cuts, -0.22, 0.18) if cuts else 1.0
    entries = jax.random.normal(stream_key, extent, jnp.float32) * width * loudness
    return jnp.minimum(jnp.maximum(entries, -bound), bound).astype(held_as)


def setup_inputs(seed: int = 0) -> dict:
    key_list = jax.random.split(jax.random.key(seed), 22)
    tokens = normal_values(key_list[0], (SEQ, D), 1.0, 6.0, ((0, 8),))
    input_gain = jnp.clip(1.0 + 0.18 * jax.random.normal(key_list[1], (D,), jnp.float32), 0.1, 1.9)
    chain_query = normal_values(key_list[2], (D, REC_KEYS), D ** -0.5, 0.125, ((0, 8), (1, 4)))
    forward_gate = normal_values(key_list[3], (D, REC_KEYS), D ** -0.5, 0.125, ((0, 8), (1, 4)))
    backward_gate = normal_values(key_list[4], (D, REC_KEYS), D ** -0.5, 0.125, ((0, 8), (1, 4)))
    chain_value = normal_values(key_list[5], (D, REC_WIDTH), D ** -0.5, 0.125, ((0, 8), (1, 4)))
    output_gate = normal_values(key_list[6], (D, REC_WIDTH), D ** -0.5, 0.125, ((0, 8), (1, 4)))
    forget_rate = jnp.clip(jnp.exp(math.log(6.0) - 3.4011974 * jax.random.uniform(key_list[7], (2, REC_KEYS), jnp.float32) ** block_levels(key_list[7], (2, REC_KEYS), ((1, 4),), -0.2, 0.2)), 0.2, 6.0)
    chain_gain = jnp.clip(1.0 + 0.18 * jax.random.normal(key_list[8], (REC_WIDTH,), jnp.float32), 0.1, 1.9)
    query_down = normal_values(key_list[9], (D, QLAT), D ** -0.5, 0.125, ((0, 8),))
    latent_down = normal_values(key_list[10], (D, KVLAT), D ** -0.5, 0.125, ((0, 8),))
    rotary_down = normal_values(key_list[11], (D, ROPE_DIM), D ** -0.5, 0.125)
    query_latent_gain = jnp.clip(1.0 + 0.18 * jax.random.normal(key_list[12], (QLAT,), jnp.float32), 0.1, 1.9)
    latent_gain = jnp.clip(1.0 + 0.18 * jax.random.normal(key_list[13], (KVLAT,), jnp.float32), 0.1, 1.9)
    query_up = normal_values(key_list[14], (QLAT, HEADS_ATT * ATT_QK), QLAT ** -0.5, 0.21875, ((1, 4),))
    latent_up = normal_values(key_list[15], (KVLAT, HEADS_ATT * (NOPE_DIM + VHEAD_DIM)), KVLAT ** -0.5, 0.25, ((1, 4),))
    query_head_gain = jnp.clip(1.0 + 0.18 * jax.random.normal(key_list[16], (ATT_QK,), jnp.float32), 0.1, 1.9)
    key_head_gain = jnp.clip(1.0 + 0.18 * jax.random.normal(key_list[17], (ATT_QK,), jnp.float32), 0.1, 1.9)
    mixer_gain = jnp.clip(1.0 + 0.18 * jax.random.normal(key_list[18], (ATT_WIDTH,), jnp.float32), 0.1, 1.9)
    chain_out = normal_values(key_list[19], (REC_WIDTH, D), (REC_WIDTH + ATT_WIDTH) ** -0.5, 0.125, ((0, 4), (1, 8)))
    attend_out = normal_values(key_list[20], (ATT_WIDTH, D), (REC_WIDTH + ATT_WIDTH) ** -0.5, 0.125, ((0, 4), (1, 8)))
    return dict(tokens=tokens, input_gain=input_gain, chain_query=chain_query, forward_gate=forward_gate, backward_gate=backward_gate, chain_value=chain_value, output_gate=output_gate, forget_rate=forget_rate, chain_gain=chain_gain, query_down=query_down, latent_down=latent_down, rotary_down=rotary_down, query_latent_gain=query_latent_gain, latent_gain=latent_gain, query_up=query_up, latent_up=latent_up, query_head_gain=query_head_gain, key_head_gain=key_head_gain, mixer_gain=mixer_gain, chain_out=chain_out, attend_out=attend_out)


norm_eps = 1e-06
rope_theta = 10000.0
finest_arithmetic_mode = lax.Precision.HIGHEST

def rms_scale(values, gain_vec):
    mean_square = lax.optimization_barrier(jnp.mean(values * values, axis=-1, keepdims=True))
    return values * lax.rsqrt(mean_square + norm_eps) * gain_vec

def rotate_tail(values, positions):
    half_dim = ROPE_DIM // 2
    inverse = rope_theta ** (-jnp.arange(0, ROPE_DIM, 2).astype(jnp.float32) / ROPE_DIM)
    angles = positions.astype(jnp.float32)[:, None] * inverse
    cosine = jnp.cos(angles)[:, None, :]
    sine_table = jnp.sin(angles)[:, None, :]
    unrotated = values[..., :NOPE_DIM]
    first_half = values[..., NOPE_DIM:NOPE_DIM + half_dim]
    latter_element = values[..., NOPE_DIM + half_dim:]
    return jnp.concatenate([unrotated, first_half * cosine - latter_element * sine_table, latter_element * cosine + first_half * sine_table], axis=-1)

def gate_parts(pre_gate, rate_row, seq_len):
    opening = rate_row / seq_len * jax.nn.sigmoid(-pre_gate.astype(jnp.float32))
    return (jnp.log1p(-opening), opening)

def summarize(query_rows, key_rows, payload_array_lines, log_decay):
    cumulative = jnp.cumsum(log_decay, axis=0)
    weighted_probe_vectors = query_rows * jnp.exp(cumulative)
    weighted_lookup_vectors = key_rows * jnp.exp(-cumulative)
    overall_shrink_multiplier = jnp.exp(cumulative[-1])
    recurrent_memory_digest = overall_shrink_multiplier[:, :, None] * jnp.einsum('jre,jrw->rew', weighted_lookup_vectors, payload_array_lines, precision=finest_arithmetic_mode)
    return (weighted_probe_vectors, weighted_lookup_vectors, overall_shrink_multiplier, recurrent_memory_digest)

def emit(weighted_probe_vectors, weighted_lookup_vectors, payload_array_lines, incoming_update):
    length = weighted_probe_vectors.shape[0]
    lower_mask = jnp.tril(jnp.ones((length, length), jnp.float32))
    scores = jnp.einsum('thk,shk->hts', weighted_probe_vectors, weighted_lookup_vectors, precision=finest_arithmetic_mode) * lower_mask
    within = jnp.einsum('hts,shv->thv', scores, payload_array_lines, precision=finest_arithmetic_mode)
    prior_state = jnp.einsum('mjf,jfi->mji', weighted_probe_vectors, incoming_update, precision=finest_arithmetic_mode)
    return within + prior_state

def run_chain(query_rows, key_rows, payload_array_lines, log_decay):
    seq_len, heads_here, key_dim = query_rows.shape
    blocks = seq_len // TOK_DEV

    def to_blocks(tensor):
        return tensor.reshape(blocks, TOK_DEV, heads_here, tensor.shape[2])

    def advance(carried, block_in):
        weighted_probe_vectors, weighted_lookup_vectors, overall_shrink_multiplier, recurrent_memory_digest = summarize(block_in[0], block_in[1], block_in[2], block_in[3])
        outputs = emit(weighted_probe_vectors, weighted_lookup_vectors, block_in[2], carried)
        return (overall_shrink_multiplier[:, :, None] * carried + recurrent_memory_digest, outputs)
    initial = jnp.zeros((heads_here, key_dim, payload_array_lines.shape[2]), jnp.float32)
    _, produced = lax.scan(advance, initial, (to_blocks(query_rows), to_blocks(key_rows), to_blocks(payload_array_lines), to_blocks(log_decay)))
    return produced.reshape(seq_len, heads_here, payload_array_lines.shape[2])

def reference(tokens, input_gain, chain_query, forward_gate, backward_gate, chain_value, output_gate, forget_rate, chain_gain, query_down, latent_down, rotary_down, query_latent_gain, latent_gain, query_up, latent_up, query_head_gain, key_head_gain, mixer_gain, chain_out, attend_out):
    seq_len = tokens.shape[0]
    normed = rms_scale(tokens.astype(jnp.float32), input_gain).astype(jnp.bfloat16)

    def project(source, weight):
        return jnp.dot(source, weight, preferred_element_type=jnp.float32).astype(jnp.bfloat16)

    def heads_of(tensor, head_width):
        return tensor.astype(jnp.float32).reshape(seq_len, tensor.shape[1] // head_width, head_width)
    query_rows = heads_of(project(normed, chain_query), KEY_DIM)
    payload_array_lines = heads_of(project(normed, chain_value), VAL_DIM)
    forward_log, forward_key = gate_parts(project(normed, forward_gate), forget_rate[0], seq_len)
    backward_log, backward_key = gate_parts(project(normed, backward_gate), forget_rate[1], seq_len)
    gate_logit = project(normed, output_gate).astype(jnp.float32)
    forward_out = run_chain(query_rows, heads_of(forward_key, KEY_DIM), payload_array_lines, heads_of(forward_log, KEY_DIM))
    reversed_out = run_chain(jnp.flip(query_rows, 0), jnp.flip(heads_of(backward_key, KEY_DIM), 0), jnp.flip(payload_array_lines, 0), jnp.flip(heads_of(backward_log, KEY_DIM), 0))
    combined = forward_out + jnp.flip(reversed_out, 0)
    head_gain = chain_gain.reshape(combined.shape[1], VAL_DIM)
    chain_mixed = (rms_scale(combined, head_gain).reshape(seq_len, -1) * jax.nn.silu(gate_logit)).astype(jnp.bfloat16)
    query_latent = rms_scale(project(normed, query_down).astype(jnp.float32), query_latent_gain).astype(jnp.bfloat16)
    pair_latent = rms_scale(project(normed, latent_down).astype(jnp.float32), latent_gain).astype(jnp.bfloat16)
    rotary_key = project(normed, rotary_down).astype(jnp.float32)
    attend_query = project(query_latent, query_up).astype(jnp.float32).reshape(seq_len, HEADS_ATT, ATT_QK)
    attend_pairs = project(pair_latent, latent_up).reshape(seq_len, HEADS_ATT, NOPE_DIM + VHEAD_DIM)
    positions = jnp.arange(seq_len, dtype=jnp.int32)
    query_final = rotate_tail(rms_scale(attend_query, query_head_gain), positions).astype(jnp.bfloat16)
    key_cat = jnp.concatenate([attend_pairs[..., :NOPE_DIM].astype(jnp.float32), jnp.broadcast_to(rotary_key[:, None, :], (seq_len, HEADS_ATT, ROPE_DIM))], axis=-1)
    key_final = rotate_tail(rms_scale(key_cat, key_head_gain), positions).astype(jnp.bfloat16)
    key_wide = key_final.astype(jnp.float32)
    value_wide = attend_pairs[..., NOPE_DIM:].astype(jnp.float32)
    score_scale = ATT_QK ** (-0.5)

    def attend(query_block):
        scores = jnp.einsum('qhd,khd->hqk', query_block.astype(jnp.float32), key_wide) * score_scale
        weights = jnp.exp(scores)
        rounded = lax.optimization_barrier(weights.astype(jnp.bfloat16)).astype(jnp.float32)
        numerator = jnp.einsum('hqk,khv->qhv', rounded, value_wide)
        return numerator / jnp.transpose(lax.optimization_barrier(jnp.sum(weights, axis=-1)))[:, :, None]
    blocks_in = query_final.reshape(seq_len // TOK_DEV, TOK_DEV, HEADS_ATT, ATT_QK)
    attend_rows = lax.map(attend, blocks_in).reshape(seq_len, HEADS_ATT, VHEAD_DIM)
    attend_mixed = rms_scale(attend_rows, mixer_gain.reshape(HEADS_ATT, VHEAD_DIM)).reshape(seq_len, ATT_WIDTH).astype(jnp.bfloat16)
    mixed_sum = jnp.dot(chain_mixed, chain_out, preferred_element_type=jnp.float32) + jnp.dot(attend_mixed, attend_out, preferred_element_type=jnp.float32)
    return mixed_sum
```

```python
import functools

import jax
import jax.numpy as jnp
from jax import lax
from jax.experimental import pallas as pl
from jax.experimental.pallas import tpu as pltpu
from jax.sharding import PartitionSpec as P

KEY_DIM = 128
VAL_DIM = 128
NOPE_DIM = 128
ROPE_DIM = 64
VHEAD_DIM = 128
ATT_QK = 192

norm_eps = 1e-06
rope_theta = 10000.0
MESH = pl.DeviceIdType.MESH
VMEM_LIMIT = 60 * 1024 * 1024
f32 = jnp.float32
bf16 = jnp.bfloat16


def rms_scale(values, gain_vec):
    mean_square = jnp.mean(values * values, axis=-1, keepdims=True)
    return values * lax.rsqrt(mean_square + norm_eps) * gain_vec


def rotate_tail(values, positions):
    half_dim = ROPE_DIM // 2
    inverse = rope_theta ** (-jnp.arange(0, ROPE_DIM, 2).astype(f32) / ROPE_DIM)
    angles = positions.astype(f32)[:, None] * inverse
    cosine = jnp.cos(angles)[:, None, :]
    sine_table = jnp.sin(angles)[:, None, :]
    unrotated = values[..., :NOPE_DIM]
    first_half = values[..., NOPE_DIM : NOPE_DIM + half_dim]
    latter = values[..., NOPE_DIM + half_dim :]
    return jnp.concatenate(
        [
            unrotated,
            first_half * cosine - latter * sine_table,
            latter * cosine + first_half * sine_table,
        ],
        axis=-1,
    )


def greet(peers):
    barrier = pltpu.get_barrier_semaphore()
    for peer in peers:
        pl.semaphore_signal(barrier, inc=1, device_id=peer, device_id_type=MESH)
    pl.semaphore_wait(barrier, len(peers))


def line_and_pair(n):
    me = lax.axis_index("sp")
    lines = n // 2
    outer, inner = me // 2, lax.rem(me, 2)
    partner = {"sp": outer * 2 + 1 - inner}

    def line_peer(d):
        return {"sp": lax.rem(outer + d, lines) * 2 + inner}

    return me, lines, outer, inner, partner, line_peer


def project_kernel(n, count, x_ref, *refs):
    weights = refs[:count]
    outs = refs[count : 2 * count]
    rest = refs[2 * count :]
    x_recv = rest[0]
    w_recv = rest[1 : 1 + count]
    p_send = rest[1 + count : 1 + 2 * count]
    p_recv = rest[1 + 2 * count : 1 + 3 * count]
    own = rest[1 + 3 * count : 1 + 4 * count]
    xs, xr, ws, wr, ps, pr = rest[1 + 4 * count :]
    me, lines, outer, inner, partner, line_peer = line_and_pair(n)
    greet([partner] + [line_peer(d) for d in range(1, lines)])

    def w_copy(c):
        return pltpu.make_async_remote_copy(
            src_ref=weights[c],
            dst_ref=w_recv[c],
            send_sem=ws.at[c],
            recv_sem=wr.at[c],
            device_id=partner,
            device_id_type=MESH,
        )

    def x_copy(d):
        return pltpu.make_async_remote_copy(
            src_ref=x_ref.at[lax.rem(outer + d, lines)],
            dst_ref=x_recv.at[d],
            send_sem=xs.at[d],
            recv_sem=xr.at[d],
            device_id=line_peer(d),
            device_id_type=MESH,
        )

    def p_copy(c, d):
        return pltpu.make_async_remote_copy(
            src_ref=p_send[c].at[d],
            dst_ref=p_recv[c].at[d],
            send_sem=ps.at[c, d],
            recv_sem=pr.at[c, d],
            device_id=line_peer(d),
            device_id_type=MESH,
        )

    for d in range(1, lines):
        x_copy(d).start()
    for c in range(count):
        w_copy(c).start()
    for c in range(count):
        w_copy(c).wait_recv()

        def part(mine, theirs):
            return jnp.dot(mine, weights[c][...], preferred_element_type=f32) + jnp.dot(
                theirs, w_recv[c][...], preferred_element_type=f32
            )

        @pl.loop(1, lines)
        def _(d):
            if c == 0:
                x_copy(d).wait_recv()
            back = lines - d
            p_send[c][back] = part(x_recv[d, inner], x_recv[d, 1 - inner]).astype(bf16)
            p_copy(c, back).start()

        own[c][...] = part(x_ref[outer, inner], x_ref[outer, 1 - inner])
    for c in range(count):

        def add(d, total):
            p_copy(c, d).wait_recv()
            return total + p_recv[c][d].astype(f32)

        outs[c][...] = lax.fori_loop(1, lines, add, own[c][...]).astype(bf16)
    for d in range(1, lines):
        x_copy(d).wait_send()
    for c in range(count):
        w_copy(c).wait_send()

        @pl.loop(1, lines)
        def _(d):
            p_copy(c, d).wait_send()


def project_all(n, x_split, weights):
    lines = n // 2
    rows, depth = x_split.shape[2:]
    count = len(weights)
    widths = [w.shape[1] for w in weights]
    vmem = pl.BlockSpec(memory_space=pltpu.VMEM)
    return pl.pallas_call(
        functools.partial(project_kernel, n, count),
        out_shape=[jax.ShapeDtypeStruct((rows, c), bf16) for c in widths],
        in_specs=[vmem] * (1 + count),
        out_specs=[vmem] * count,
        scratch_shapes=[pltpu.VMEM((lines, 2, rows, depth), bf16)]
        + [pltpu.VMEM((depth, c), bf16) for c in widths]
        + [pltpu.VMEM((lines, rows, c), bf16) for c in widths]
        + [pltpu.VMEM((lines, rows, c), bf16) for c in widths]
        + [pltpu.VMEM((rows, c), f32) for c in widths]
        + [
            pltpu.SemaphoreType.DMA((lines,)),
            pltpu.SemaphoreType.DMA((lines,)),
            pltpu.SemaphoreType.DMA((count,)),
            pltpu.SemaphoreType.DMA((count,)),
            pltpu.SemaphoreType.DMA((count, lines)),
            pltpu.SemaphoreType.DMA((count, lines)),
        ],
        compiler_params=pltpu.CompilerParams(
            collective_id=0, has_side_effects=True, vmem_limit_bytes=VMEM_LIMIT
        ),
    )(x_split, *weights)


def gather_kernel(n, count, *refs):
    ins, outs = refs[:count], refs[count : 2 * count]
    keep, s1, r1, s2, r2 = refs[2 * count :]
    me, lines, outer, inner, partner, line_peer = line_and_pair(n)
    greet([partner] + [line_peer(d) for d in range(1, lines)])

    def along(k, d):
        return pltpu.make_async_remote_copy(
            src_ref=ins[k],
            dst_ref=outs[k].at[me],
            send_sem=s1.at[k, d],
            recv_sem=r1.at[k, d],
            device_id=line_peer(d),
            device_id_type=MESH,
        )

    def across(k, d):
        slot = lax.rem(outer - d + lines, lines) * 2 + inner
        return pltpu.make_async_remote_copy(
            src_ref=ins[k] if isinstance(d, int) and d == 0 else outs[k].at[slot],
            dst_ref=outs[k].at[slot],
            send_sem=s2.at[k, d],
            recv_sem=r2.at[k, d],
            device_id=partner,
            device_id_type=MESH,
        )

    def local(k):
        return pltpu.make_async_copy(ins[k], outs[k].at[me], keep.at[k])

    for k in range(count):

        @pl.loop(1, lines)
        def _(d):
            along(k, d).start()

        across(k, 0).start()
        local(k).start()
    for k in range(count):

        @pl.loop(1, lines)
        def _(d):
            along(k, d).wait_recv()
            across(k, d).start()

    for k in range(count):
        local(k).wait()
        across(k, 0).wait()

        @pl.loop(1, lines)
        def _(d):
            along(k, d).wait_send()
            across(k, d).wait()


def gather_all(n, blocks):
    lines = n // 2
    count = len(blocks)
    vmem = pl.BlockSpec(memory_space=pltpu.VMEM)
    return pl.pallas_call(
        functools.partial(gather_kernel, n, count),
        out_shape=[jax.ShapeDtypeStruct((n,) + b.shape, b.dtype) for b in blocks],
        in_specs=[vmem] * count,
        out_specs=[vmem] * count,
        scratch_shapes=[pltpu.SemaphoreType.DMA((count,))]
        + [pltpu.SemaphoreType.DMA((count, lines))] * 4,
        compiler_params=pltpu.CompilerParams(
            collective_id=1, has_side_effects=True, vmem_limit_bytes=VMEM_LIMIT
        ),
    )(*blocks)


def heads_peer(n, d):
    return {"tp": lax.rem(lax.axis_index("tp") + d, n)}


def latent_kernel(n, in_ref, out_ref, ss, rs, keep):
    me = lax.axis_index("tp")
    greet([heads_peer(n, d) for d in range(1, n)])

    def copy(d):
        return pltpu.make_async_remote_copy(
            src_ref=in_ref,
            dst_ref=out_ref.at[me],
            send_sem=ss.at[d],
            recv_sem=rs.at[d],
            device_id=heads_peer(n, d),
            device_id_type=MESH,
        )

    for d in range(1, n):
        copy(d).start()
    stay = pltpu.make_async_copy(in_ref, out_ref.at[me], keep)
    stay.start()
    stay.wait()
    for d in range(1, n):
        copy(d).wait()


def gather_heads(n, block):
    vmem = pl.BlockSpec(memory_space=pltpu.VMEM)
    return pl.pallas_call(
        functools.partial(latent_kernel, n),
        out_shape=jax.ShapeDtypeStruct((n,) + block.shape, block.dtype),
        in_specs=[vmem],
        out_specs=vmem,
        scratch_shapes=[
            pltpu.SemaphoreType.DMA((n,)),
            pltpu.SemaphoreType.DMA((n,)),
            pltpu.SemaphoreType.DMA,
        ],
        compiler_params=pltpu.CompilerParams(collective_id=2, has_side_effects=True),
    )(block)


def output_kernel(n, mix_ref, w_ref, out_ref, send, recv, ss, rs):
    me = lax.axis_index("tp")
    greet([heads_peer(n, d) for d in range(1, n)])

    def copy(d):
        return pltpu.make_async_remote_copy(
            src_ref=send.at[d],
            dst_ref=recv.at[d],
            send_sem=ss.at[d],
            recv_sem=rs.at[d],
            device_id=heads_peer(n, d),
            device_id_type=MESH,
        )

    for d in range(1, n):
        rows = mix_ref[lax.rem(me + d, n)]
        send[d] = jnp.dot(rows, w_ref[...], preferred_element_type=f32).astype(bf16)
        copy(d).start()
    total = jnp.dot(mix_ref[me], w_ref[...], preferred_element_type=f32)
    for d in range(1, n):
        copy(d).wait_recv()
        total = total + recv[d].astype(f32)
    out_ref[...] = total
    for d in range(1, n):
        copy(d).wait_send()


def output_all(n, mix, weight):
    rows, cols = mix.shape[1], weight.shape[1]
    vmem = pl.BlockSpec(memory_space=pltpu.VMEM)
    return pl.pallas_call(
        functools.partial(output_kernel, n),
        out_shape=jax.ShapeDtypeStruct((rows, cols), f32),
        in_specs=[vmem] * 2,
        out_specs=vmem,
        scratch_shapes=[
            pltpu.VMEM((n, rows, cols), bf16),
            pltpu.VMEM((n, rows, cols), bf16),
            pltpu.SemaphoreType.DMA((n,)),
            pltpu.SemaphoreType.DMA((n,)),
        ],
        compiler_params=pltpu.CompilerParams(
            collective_id=3, has_side_effects=True, vmem_limit_bytes=VMEM_LIMIT
        ),
    )(mix, weight)


def gate_parts(pre_gate, rate_row, seq_len):
    opening = rate_row / seq_len * jax.nn.sigmoid(-pre_gate.astype(f32))
    return (jnp.log1p(-opening), opening)


def on_device(
    tokens,
    input_gain,
    chain_query,
    forward_gate,
    backward_gate,
    chain_value,
    output_gate,
    forget_rate,
    chain_gain,
    query_down,
    latent_down,
    rotary_down,
    query_latent_gain,
    latent_gain,
    query_up,
    latent_up,
    query_head_gain,
    key_head_gain,
    mixer_gain,
    chain_out,
    attend_out,
):
    n_sp, n_tp = lax.axis_size("sp"), lax.axis_size("tp")
    sp, tp = lax.axis_index("sp"), lax.axis_index("tp")
    rows, depth = tokens.shape[0], chain_query.shape[0]
    seq_len = rows * n_sp
    q_cols = query_down.shape[1] // n_tp
    l_cols = latent_down.shape[1] // n_tp
    down = jnp.concatenate(
        [
            lax.dynamic_slice_in_dim(query_down, tp * q_cols, q_cols, 1),
            lax.dynamic_slice_in_dim(latent_down, tp * l_cols, l_cols, 1),
        ],
        axis=1,
    )
    normed = rms_scale(tokens.astype(f32), input_gain).astype(bf16)
    x_split = normed.reshape(rows, n_sp // 2, 2, depth).transpose(1, 2, 0, 3)
    raw, q_rows, fwd_logit, bwd_logit, v_rows, gate_logit = project_all(
        n_sp, x_split, (down, chain_query, forward_gate, backward_gate, chain_value, output_gate)
    )

    def project(source, weight):
        return jnp.dot(source, weight, preferred_element_type=f32).astype(bf16)

    all_raw = gather_heads(n_tp, raw)
    raw_q = all_raw[:, :, :q_cols].transpose(1, 0, 2).reshape(rows, -1).astype(f32)
    raw_l = all_raw[:, :, q_cols:].transpose(1, 0, 2).reshape(rows, -1).astype(f32)
    query_latent = rms_scale(raw_q, query_latent_gain).astype(bf16)
    pair_latent = rms_scale(raw_l, latent_gain).astype(bf16)
    rotary_key = project(normed, rotary_down).astype(f32)
    heads = query_up.shape[1] // ATT_QK
    attend_query = project(query_latent, query_up).astype(f32).reshape(rows, heads, ATT_QK)
    attend_pairs = project(pair_latent, latent_up).reshape(rows, heads, NOPE_DIM + VHEAD_DIM)
    positions = sp * rows + jnp.arange(rows, dtype=jnp.int32)
    query_final = rotate_tail(rms_scale(attend_query, query_head_gain), positions).astype(bf16)
    key_cat = jnp.concatenate(
        [
            attend_pairs[..., :NOPE_DIM].astype(f32),
            jnp.broadcast_to(rotary_key[:, None, :], (rows, heads, ROPE_DIM)),
        ],
        axis=-1,
    )
    key_final = rotate_tail(rms_scale(key_cat, key_head_gain), positions).astype(bf16)
    keys_flat = key_final.reshape(rows, heads * ATT_QK)
    values_flat = attend_pairs[..., NOPE_DIM:].reshape(rows, heads * VHEAD_DIM)

    f_log, f_key = gate_parts(fwd_logit, forget_rate[0], seq_len)
    b_log, b_key = gate_parts(bwd_logit, forget_rate[1], seq_len)
    width = f_log.shape[1]
    chain_heads = width // KEY_DIM
    lower = jnp.tril(jnp.ones((rows, rows), f32))
    f_cum = jnp.dot(lower, f_log, precision=lax.Precision.HIGHEST)
    b_cum = jnp.dot(lower.T, b_log, precision=lax.Precision.HIGHEST)
    q_wide = q_rows.astype(f32)

    def by_head(tensor):
        return tensor.astype(bf16).reshape(rows, chain_heads, -1)

    f_q, f_k = by_head(q_wide * jnp.exp(f_cum)), by_head(f_key * jnp.exp(-f_cum))
    b_q, b_k = by_head(q_wide * jnp.exp(b_cum)), by_head(b_key * jnp.exp(-b_cum))
    v_heads = v_rows.reshape(rows, chain_heads, VAL_DIM)
    logs = jnp.stack([f_cum[-1], b_cum[0]])

    def digest(keys, log):
        state = jnp.einsum("jre,jrw->rew", keys, v_heads, preferred_element_type=f32)
        return state * jnp.exp(log).reshape(chain_heads, KEY_DIM, 1)

    states = jnp.stack([digest(f_k, logs[0]), digest(b_k, logs[1])]).astype(bf16)
    own_out = jnp.concatenate([chain_out, attend_out], axis=0)

    all_keys, all_values, all_states, all_logs, all_out = gather_all(
        n_sp,
        (keys_flat, values_flat, states.reshape(2 * width, VAL_DIM), logs, own_out),
    )

    index = jnp.arange(n_sp)
    before = (index < sp)[:, None]
    after = (index > sp)[:, None]
    between_f = ((index[None, :] > index[:, None]) & (index[None, :] < sp)).astype(f32)
    between_b = ((index[None, :] < index[:, None]) & (index[None, :] > sp)).astype(f32)
    sum_f = jnp.sum(between_f[:, :, None] * all_logs[None, :, 0], axis=1)
    sum_b = jnp.sum(between_b[:, :, None] * all_logs[None, :, 1], axis=1)
    coef = jnp.stack(
        [jnp.where(before, jnp.exp(sum_f), 0.0), jnp.where(after, jnp.exp(sum_b), 0.0)], axis=1
    ).reshape(n_sp, 2 * width, 1)
    entering = jnp.sum(coef * all_states.astype(f32), axis=0).astype(bf16)
    entering = entering.reshape(2, chain_heads, KEY_DIM, VAL_DIM)

    def scores(queries, keys, mask):
        return (
            jnp.einsum("thk,shk->hts", queries, keys, preferred_element_type=f32) * mask
        )

    both = (scores(f_q, f_k, lower) + scores(b_q, b_k, lower.T)).astype(bf16)
    combined = (
        jnp.einsum("hts,shv->thv", both, v_heads, preferred_element_type=f32)
        + jnp.einsum("thk,hkv->thv", f_q, entering[0], preferred_element_type=f32)
        + jnp.einsum("thk,hkv->thv", b_q, entering[1], preferred_element_type=f32)
    )
    head_gain = chain_gain.reshape(chain_heads, VAL_DIM)
    chain_mixed = (
        rms_scale(combined, head_gain).reshape(rows, -1) * jax.nn.silu(gate_logit.astype(f32))
    ).astype(bf16)

    key_all = all_keys.reshape(seq_len, heads, ATT_QK)
    value_all = all_values.reshape(seq_len, heads, VHEAD_DIM)
    weights = jnp.exp(
        jnp.einsum("qhd,khd->hqk", query_final, key_all, preferred_element_type=f32)
        * ATT_QK ** (-0.5)
    )
    numerator = jnp.einsum(
        "hqk,khv->qhv", weights.astype(bf16), value_all, preferred_element_type=f32
    )
    denominator = jnp.sum(weights, axis=-1)
    attend_rows = numerator / jnp.transpose(denominator)[:, :, None]
    attend_mixed = (
        rms_scale(attend_rows, mixer_gain.reshape(heads, VHEAD_DIM))
        .reshape(rows, heads * VHEAD_DIM)
        .astype(bf16)
    )
    mix = jnp.concatenate([chain_mixed, attend_mixed], axis=1)
    full_out = all_out.transpose(1, 0, 2).reshape(mix.shape[1], -1)
    return output_all(n_tp, mix.reshape(n_tp, rows // n_tp, -1), full_out)


def solution(mesh):
    placed = (
        P("sp", None),
        P(),
        P("sp", "tp"),
        P("sp", "tp"),
        P("sp", "tp"),
        P("sp", "tp"),
        P("sp", "tp"),
        P(None, "tp"),
        P("tp"),
        P("sp", None),
        P("sp", None),
        P(),
        P(),
        P(),
        P(None, "tp"),
        P(None, "tp"),
        P(),
        P(),
        P("tp"),
        P("tp", "sp"),
        P("tp", "sp"),
    )
    return jax.shard_map(
        on_device, mesh=mesh, in_specs=placed, out_specs=P(("sp", "tp"), None), check_vma=False
    )
```

```python
import functools

import jax
import jax.numpy as jnp
from jax import lax
from jax.experimental import pallas as pl
from jax.experimental.pallas import tpu as pltpu
from jax.sharding import PartitionSpec as P

KEY_DIM = 128
VAL_DIM = 128
NOPE_DIM = 128
ROPE_DIM = 64
VHEAD_DIM = 128
ATT_QK = 192

norm_eps = 1e-06
rope_theta = 10000.0
MESH = pl.DeviceIdType.MESH
VMEM_LIMIT = 60 * 1024 * 1024
f32 = jnp.float32
bf16 = jnp.bfloat16


def rms_scale(values, gain_vec):
    mean_square = jnp.mean(values * values, axis=-1, keepdims=True)
    return values * lax.rsqrt(mean_square + norm_eps) * gain_vec


def rotate_tail(values, positions):
    half_dim = ROPE_DIM // 2
    inverse = rope_theta ** (-jnp.arange(0, ROPE_DIM, 2).astype(f32) / ROPE_DIM)
    angles = positions.astype(f32)[:, None] * inverse
    cosine = jnp.cos(angles)[:, None, :]
    sine_table = jnp.sin(angles)[:, None, :]
    unrotated = values[..., :NOPE_DIM]
    first_half = values[..., NOPE_DIM : NOPE_DIM + half_dim]
    latter = values[..., NOPE_DIM + half_dim :]
    return jnp.concatenate(
        [
            unrotated,
            first_half * cosine - latter * sine_table,
            latter * cosine + first_half * sine_table,
        ],
        axis=-1,
    )


def greet(peers):
    barrier = pltpu.get_barrier_semaphore()
    for peer in peers:
        pl.semaphore_signal(barrier, inc=1, device_id=peer, device_id_type=MESH)
    pl.semaphore_wait(barrier, len(peers))


def line_and_pair(n):
    me = lax.axis_index("sp")
    lines = n // 2
    outer, inner = me // 2, lax.rem(me, 2)
    partner = {"sp": outer * 2 + 1 - inner}

    def line_peer(d):
        return {"sp": lax.rem(outer + d, lines) * 2 + inner}

    return me, lines, outer, inner, partner, line_peer


def project_kernel(n, count, x_ref, *refs):
    weights = refs[:count]
    outs = refs[count : 2 * count]
    rest = refs[2 * count :]
    x_recv = rest[0]
    w_recv = rest[1 : 1 + count]
    p_send = rest[1 + count : 1 + 2 * count]
    p_recv = rest[1 + 2 * count : 1 + 3 * count]
    own = rest[1 + 3 * count : 1 + 4 * count]
    xs, xr, ws, wr, ps, pr = rest[1 + 4 * count :]
    groups = n // 4
    me = lax.axis_index("sp")
    group, place = me // 4, lax.rem(me, 4)
    low, inner = place // 2, lax.rem(place, 2)
    places = (
        place,
        (1 - low) * 2 + inner,
        low * 2 + 1 - inner,
        (1 - low) * 2 + 1 - inner,
    )
    beside = {"sp": group * 4 + places[1]}
    partner = {"sp": group * 4 + places[2]}

    def far_peer(d):
        return {"sp": lax.rem(group + d, groups) * 4 + place}

    greet([beside, partner] + [far_peer(d) for d in range(1, groups)])

    def w_copy(c, k):
        return pltpu.make_async_remote_copy(
            src_ref=w_recv[c].at[0] if k == 2 else weights[c],
            dst_ref=w_recv[c].at[k],
            send_sem=ws.at[c, k],
            recv_sem=wr.at[c, k],
            device_id=beside if k == 0 else partner,
            device_id_type=MESH,
        )

    def x_copy(d):
        return pltpu.make_async_remote_copy(
            src_ref=x_ref.at[lax.rem(group + d, groups)],
            dst_ref=x_recv.at[d],
            send_sem=xs.at[d],
            recv_sem=xr.at[d],
            device_id=far_peer(d),
            device_id_type=MESH,
        )

    def p_copy(c, d):
        return pltpu.make_async_remote_copy(
            src_ref=p_send[c].at[d],
            dst_ref=p_recv[c].at[d],
            send_sem=ps.at[c, d],
            recv_sem=pr.at[c, d],
            device_id=far_peer(d),
            device_id_type=MESH,
        )

    w_copy(0, 0).start()
    w_copy(0, 1).start()
    for d in range(1, groups):
        x_copy(d).start()
    for c in range(1, count):
        w_copy(c, 0).start()
    for c in range(count):
        w_copy(c, 0).wait_recv()
        w_copy(c, 2).start()
        if c + 1 < count:
            w_copy(c + 1, 1).start()
    for c in range(count):
        w_copy(c, 1).wait_recv()
        w_copy(c, 2).wait_recv()

        def part(x):
            total = jnp.dot(x(places[0]), weights[c][...], preferred_element_type=f32)
            for k in range(3):
                total += jnp.dot(x(places[k + 1]), w_recv[c][k], preferred_element_type=f32)
            return total

        @pl.loop(1, groups)
        def _(d):
            if c == 0:
                x_copy(d).wait_recv()
            back = groups - d
            p_send[c][back] = part(lambda k: x_recv[d, k]).astype(bf16)
            p_copy(c, back).start()

        own[c][...] = part(lambda k: x_ref[group, k])
    for c in range(count):

        def add(d, total):
            p_copy(c, d).wait_recv()
            return total + p_recv[c][d].astype(f32)

        outs[c][...] = lax.fori_loop(1, groups, add, own[c][...]).astype(bf16)
    for d in range(1, groups):
        x_copy(d).wait_send()
    for c in range(count):
        for k in range(3):
            w_copy(c, k).wait_send()

        @pl.loop(1, groups)
        def _(d):
            p_copy(c, d).wait_send()


def project_all(n, x_split, weights):
    groups = n // 4
    rows, depth = x_split.shape[2:]
    count = len(weights)
    widths = [w.shape[1] for w in weights]
    vmem = pl.BlockSpec(memory_space=pltpu.VMEM)
    return pl.pallas_call(
        functools.partial(project_kernel, n, count),
        out_shape=[jax.ShapeDtypeStruct((rows, c), bf16) for c in widths],
        in_specs=[vmem] * (1 + count),
        out_specs=[vmem] * count,
        scratch_shapes=[pltpu.VMEM((groups, 4, rows, depth), bf16)]
        + [pltpu.VMEM((3, depth, c), bf16) for c in widths]
        + [pltpu.VMEM((groups, rows, c), bf16) for c in widths]
        + [pltpu.VMEM((groups, rows, c), bf16) for c in widths]
        + [pltpu.VMEM((rows, c), f32) for c in widths]
        + [
            pltpu.SemaphoreType.DMA((groups,)),
            pltpu.SemaphoreType.DMA((groups,)),
            pltpu.SemaphoreType.DMA((count, 3)),
            pltpu.SemaphoreType.DMA((count, 3)),
            pltpu.SemaphoreType.DMA((count, groups)),
            pltpu.SemaphoreType.DMA((count, groups)),
        ],
        compiler_params=pltpu.CompilerParams(
            collective_id=0, has_side_effects=True, vmem_limit_bytes=VMEM_LIMIT
        ),
    )(x_split, *weights)


def gather_kernel(n, heads_n, *refs):
    count = 5
    query_in, pair_in, ins = refs[0], refs[1], refs[2 : 2 + count]
    query_out, pair_out, outs = refs[2 + count], refs[3 + count], refs[4 + count : 4 + 2 * count]
    keep, s1, r1, s2, r2, hs1, hr1, hs2, hr2 = refs[4 + 2 * count :]
    me, lines, outer, inner, partner, line_peer = line_and_pair(n)
    head = lax.axis_index("tp")
    head_lines = heads_n // 2
    head_outer, head_inner = head // 2, lax.rem(head, 2)
    head_partner = {"tp": head_outer * 2 + 1 - head_inner}

    def head_peer(d):
        return {"tp": lax.rem(head_outer + d, head_lines) * 2 + head_inner}

    greet(
        [partner, head_partner]
        + [line_peer(d) for d in range(1, lines)]
        + [head_peer(d) for d in range(1, head_lines)]
    )
    src = (pair_in,) + tuple(ins)

    def slot(k, at):
        return pair_out.at[head, at] if k == 0 else outs[k - 1].at[at]

    def along(k, d):
        return pltpu.make_async_remote_copy(
            src_ref=src[k],
            dst_ref=slot(k, me),
            send_sem=s1.at[k, d],
            recv_sem=r1.at[k, d],
            device_id=line_peer(d),
            device_id_type=MESH,
        )

    def across(k, d):
        at = lax.rem(outer - d + lines, lines) * 2 + inner
        return pltpu.make_async_remote_copy(
            src_ref=src[k] if isinstance(d, int) and d == 0 else slot(k, at),
            dst_ref=slot(k, at),
            send_sem=s2.at[k, d],
            recv_sem=r2.at[k, d],
            device_id=partner,
            device_id_type=MESH,
        )

    def local(k):
        return pltpu.make_async_copy(src[k], slot(k, me), keep.at[k])

    def head_along(j, d):
        return pltpu.make_async_remote_copy(
            src_ref=query_in if j == 0 else pair_out.at[head],
            dst_ref=query_out.at[head] if j == 0 else pair_out.at[head],
            send_sem=hs1.at[j, d],
            recv_sem=hr1.at[j, d],
            device_id=head_peer(d),
            device_id_type=MESH,
        )

    def head_across(j, d):
        at = lax.rem(head_outer - d + head_lines, head_lines) * 2 + head_inner
        own = isinstance(d, int) and d == 0
        out = query_out if j == 0 else pair_out
        return pltpu.make_async_remote_copy(
            src_ref=query_in if j == 0 and own else out.at[at],
            dst_ref=out.at[at],
            send_sem=hs2.at[j, d],
            recv_sem=hr2.at[j, d],
            device_id=head_partner,
            device_id_type=MESH,
        )

    query_local = pltpu.make_async_copy(query_in, query_out.at[head], keep.at[1 + count])

    def needed(k, there):
        if k == 2:
            return there
        if k == 3:
            return jnp.logical_not(there)
        return None

    def maybe(condition, act):
        if condition is None:
            act()
        else:
            pl.when(condition)(act)

    def on_line(k, sending, act):
        @pl.loop(1, lines)
        def _(d):
            there = outer + d < lines if sending else outer >= d
            maybe(needed(k, there), lambda: act(d))

    for k in range(1 + count):
        on_line(k, True, lambda d: along(k, d).start())
        across(k, 0).start()
        local(k).start()
        if k == 0:
            for d in range(1, head_lines):
                head_along(0, d).start()
            head_across(0, 0).start()
            query_local.start()

    def pass_on(k):
        def act(d):
            along(k, d).wait_recv()
            across(k, d).start()

        on_line(k, False, act)

    pass_on(0)
    for d in range(1, head_lines):
        head_along(0, d).wait_recv()
        head_across(0, d).start()
    local(0).wait()
    across(0, 0).wait_recv()
    on_line(0, False, lambda d: across(0, d).wait_recv())
    for d in range(1, head_lines):
        head_along(1, d).start()
    head_across(1, 0).start()
    for k in range(1, count - 1):
        pass_on(k)
    for d in range(1, head_lines):
        head_along(1, d).wait_recv()
        head_across(1, d).start()
    for k in range(count - 1, 1 + count):
        pass_on(k)

    query_local.wait()
    for k in range(1 + count):
        across(k, 0).wait_send()
        if k > 0:
            local(k).wait()
            across(k, 0).wait_recv()
        on_line(k, True, lambda d: along(k, d).wait_send())

        def act(d):
            across(k, d).wait_send()
            if k > 0:
                across(k, d).wait_recv()

        on_line(k, False, act)
    for j in range(2):
        head_across(j, 0).wait()
        for d in range(1, head_lines):
            head_along(j, d).wait_send()
            head_across(j, d).wait()


def gather_all(n, heads_n, query, pair, blocks):
    lines, head_lines = n // 2, heads_n // 2
    count = len(blocks)
    vmem = pl.BlockSpec(memory_space=pltpu.VMEM)
    return pl.pallas_call(
        functools.partial(gather_kernel, n, heads_n),
        out_shape=[
            jax.ShapeDtypeStruct((heads_n,) + query.shape, query.dtype),
            jax.ShapeDtypeStruct((heads_n, n) + pair.shape, pair.dtype),
        ]
        + [jax.ShapeDtypeStruct((n,) + b.shape, b.dtype) for b in blocks],
        in_specs=[vmem] * (2 + count),
        out_specs=[vmem] * (2 + count),
        scratch_shapes=[pltpu.SemaphoreType.DMA((2 + count,))]
        + [pltpu.SemaphoreType.DMA((1 + count, lines))] * 4
        + [pltpu.SemaphoreType.DMA((2, head_lines))] * 4,
        compiler_params=pltpu.CompilerParams(
            collective_id=1, has_side_effects=True, vmem_limit_bytes=VMEM_LIMIT
        ),
    )(query, pair, *blocks)


def heads_peer(n, d):
    return {"tp": lax.rem(lax.axis_index("tp") + d, n)}


def output_kernel(n, chain_ref, attend_ref, wc_ref, wa_ref, out_ref, send, recv, ss, rs):
    me = lax.axis_index("tp")
    greet([heads_peer(n, d) for d in range(1, n)])

    def copy(d):
        return pltpu.make_async_remote_copy(
            src_ref=send.at[d],
            dst_ref=recv.at[d],
            send_sem=ss.at[d],
            recv_sem=rs.at[d],
            device_id=heads_peer(n, d),
            device_id_type=MESH,
        )

    def rows_of(at):
        chain, attend = chain_ref[at], attend_ref[at]
        return jnp.concatenate(
            [
                jnp.dot(chain, wc_ref[s], preferred_element_type=f32)
                + jnp.dot(attend, wa_ref[s], preferred_element_type=f32)
                for s in range(wc_ref.shape[0])
            ],
            axis=1,
        )

    for d in range(1, n):
        send[d] = rows_of(lax.rem(me + d, n)).astype(bf16)
        copy(d).start()
    total = rows_of(me)
    for d in range(1, n):
        copy(d).wait_recv()
        total = total + recv[d].astype(f32)
    out_ref[...] = total
    for d in range(1, n):
        copy(d).wait_send()


def output_all(n, chain, attend, chain_w, attend_w):
    rows, cols = chain.shape[1], chain_w.shape[0] * chain_w.shape[2]
    vmem = pl.BlockSpec(memory_space=pltpu.VMEM)
    return pl.pallas_call(
        functools.partial(output_kernel, n),
        out_shape=jax.ShapeDtypeStruct((rows, cols), f32),
        in_specs=[vmem] * 4,
        out_specs=vmem,
        scratch_shapes=[
            pltpu.VMEM((n, rows, cols), bf16),
            pltpu.VMEM((n, rows, cols), bf16),
            pltpu.SemaphoreType.DMA((n,)),
            pltpu.SemaphoreType.DMA((n,)),
        ],
        compiler_params=pltpu.CompilerParams(
            collective_id=3, has_side_effects=True, vmem_limit_bytes=VMEM_LIMIT
        ),
    )(chain, attend, chain_w, attend_w)


def gate_parts(pre_gate, rate_row, seq_len):
    opening = rate_row / seq_len * jax.nn.sigmoid(-pre_gate.astype(f32))
    return (jnp.log1p(-opening), opening)


def on_device(
    tokens,
    input_gain,
    chain_query,
    forward_gate,
    backward_gate,
    chain_value,
    output_gate,
    forget_rate,
    chain_gain,
    query_down,
    latent_down,
    rotary_down,
    query_latent_gain,
    latent_gain,
    query_up,
    latent_up,
    query_head_gain,
    key_head_gain,
    mixer_gain,
    chain_out,
    attend_out,
):
    n_sp, n_tp = lax.axis_size("sp"), lax.axis_size("tp")
    sp, tp = lax.axis_index("sp"), lax.axis_index("tp")
    rows, depth = tokens.shape[0], chain_query.shape[0]
    seq_len = rows * n_sp
    q_cols = query_down.shape[1] // n_tp
    l_cols = latent_down.shape[1] // n_tp
    r_cols = ROPE_DIM // n_tp
    q_down = lax.dynamic_slice_in_dim(query_down, tp * q_cols, q_cols, 1)
    l_down = jnp.concatenate(
        [
            lax.dynamic_slice_in_dim(latent_down, tp * l_cols, l_cols, 1),
            lax.dynamic_slice(rotary_down, (sp * depth, tp * r_cols), (depth, r_cols)),
        ],
        axis=1,
    )
    normed = rms_scale(tokens.astype(f32), input_gain).astype(bf16)
    x_split = normed.reshape(rows, n_sp // 4, 4, depth).transpose(1, 2, 0, 3)
    raw_q, raw_l, q_rows, fwd_logit, bwd_logit, v_rows, gate_logit = project_all(
        n_sp,
        x_split,
        (q_down, l_down, chain_query, forward_gate, backward_gate, chain_value, output_gate),
    )

    def project(source, weight):
        return jnp.dot(source, weight, preferred_element_type=f32).astype(bf16)

    f_log, f_key = gate_parts(fwd_logit, forget_rate[0], seq_len)
    b_log, b_key = gate_parts(bwd_logit, forget_rate[1], seq_len)
    width = f_log.shape[1]
    chain_heads = width // KEY_DIM
    lower = jnp.tril(jnp.ones((rows, rows), f32))
    f_cum = jnp.dot(lower, f_log, precision=lax.Precision.HIGHEST)
    b_cum = jnp.dot(lower.T, b_log, precision=lax.Precision.HIGHEST)
    q_wide = q_rows.astype(f32)

    def by_head(tensor):
        return tensor.astype(bf16).reshape(rows, chain_heads, -1)

    f_q, f_k = by_head(q_wide * jnp.exp(f_cum)), by_head(f_key * jnp.exp(-f_cum))
    b_q, b_k = by_head(q_wide * jnp.exp(b_cum)), by_head(b_key * jnp.exp(-b_cum))
    v_heads = v_rows.reshape(rows, chain_heads, VAL_DIM)
    logs = jnp.stack([f_cum[-1], b_cum[0]])

    def digest(keys, log):
        state = jnp.einsum("jre,jrw->rew", keys, v_heads, preferred_element_type=f32)
        return state * jnp.exp(log).reshape(chain_heads, KEY_DIM, 1)

    f_state, b_state = digest(f_k, logs[0]).astype(bf16), digest(b_k, logs[1]).astype(bf16)

    query_raw, pair_raw, all_logs, all_f, all_b, all_chain, all_attend = gather_all(
        n_sp,
        n_tp,
        raw_q,
        raw_l,
        (
            logs,
            f_state.reshape(width, VAL_DIM),
            b_state.reshape(width, VAL_DIM),
            chain_out,
            attend_out,
        ),
    )

    index = jnp.arange(n_sp)
    before = (index < sp)[:, None]
    after = (index > sp)[:, None]
    between_f = ((index[None, :] > index[:, None]) & (index[None, :] < sp)).astype(f32)
    between_b = ((index[None, :] < index[:, None]) & (index[None, :] > sp)).astype(f32)
    sum_f = jnp.sum(between_f[:, :, None] * all_logs[None, :, 0], axis=1)
    sum_b = jnp.sum(between_b[:, :, None] * all_logs[None, :, 1], axis=1)
    def entering(mask, log_sum, states):
        wide = jnp.exp(log_sum)[:, :, None] * states.astype(f32)
        total = jnp.sum(jnp.where(mask[:, :, None], wide, 0.0), axis=0)
        return total.astype(bf16).reshape(chain_heads, KEY_DIM, VAL_DIM)

    f_in, b_in = entering(before, sum_f, all_f), entering(after, sum_b, all_b)

    def scores(queries, keys, mask):
        return (
            jnp.einsum("thk,shk->hts", queries, keys, preferred_element_type=f32) * mask
        )

    both = (scores(f_q, f_k, lower) + scores(b_q, b_k, lower.T)).astype(bf16)
    combined = (
        jnp.einsum("hts,shv->thv", both, v_heads, preferred_element_type=f32)
        + jnp.einsum("thk,hkv->thv", f_q, f_in, preferred_element_type=f32)
        + jnp.einsum("thk,hkv->thv", b_q, b_in, preferred_element_type=f32)
    )
    head_gain = chain_gain.reshape(chain_heads, VAL_DIM)
    chain_mixed = (
        rms_scale(combined, head_gain).reshape(rows, -1) * jax.nn.silu(gate_logit.astype(f32))
    ).astype(bf16)

    heads = query_up.shape[1] // ATT_QK
    query_latent = rms_scale(
        query_raw.transpose(1, 0, 2).reshape(rows, -1).astype(f32), query_latent_gain
    ).astype(bf16)
    pair_rows = pair_raw.transpose(1, 2, 0, 3)
    pair_latent = rms_scale(
        pair_rows[..., :l_cols].reshape(seq_len, -1).astype(f32), latent_gain
    ).astype(bf16)
    rotary_key = pair_rows[..., l_cols:].reshape(seq_len, ROPE_DIM).astype(f32)
    attend_query = project(query_latent, query_up).astype(f32).reshape(rows, heads, ATT_QK)
    attend_pairs = project(pair_latent, latent_up).reshape(seq_len, heads, NOPE_DIM + VHEAD_DIM)
    query_final = rotate_tail(
        rms_scale(attend_query, query_head_gain), sp * rows + jnp.arange(rows, dtype=jnp.int32)
    ).astype(bf16)
    key_cat = jnp.concatenate(
        [
            attend_pairs[..., :NOPE_DIM].astype(f32),
            jnp.broadcast_to(rotary_key[:, None, :], (seq_len, heads, ROPE_DIM)),
        ],
        axis=-1,
    )
    key_all = rotate_tail(
        rms_scale(key_cat, key_head_gain), jnp.arange(seq_len, dtype=jnp.int32)
    ).astype(bf16)
    value_all = attend_pairs[..., NOPE_DIM:]
    weights = jnp.exp(
        jnp.einsum("qhd,khd->hqk", query_final, key_all, preferred_element_type=f32)
        * ATT_QK ** (-0.5)
    )
    numerator = jnp.einsum(
        "hqk,khv->qhv", weights.astype(bf16), value_all, preferred_element_type=f32
    )
    denominator = jnp.sum(weights, axis=-1)
    attend_rows = numerator / jnp.transpose(denominator)[:, :, None]
    attend_mixed = (
        rms_scale(attend_rows, mixer_gain.reshape(heads, VHEAD_DIM))
        .reshape(rows, heads * VHEAD_DIM)
        .astype(bf16)
    )
    def row_blocks(tensor):
        return tensor.reshape(n_tp, rows // n_tp, -1)

    return output_all(
        n_tp, row_blocks(chain_mixed), row_blocks(attend_mixed), all_chain, all_attend
    )


def solution(mesh):
    placed = (
        P("sp", None),
        P(),
        P("sp", "tp"),
        P("sp", "tp"),
        P("sp", "tp"),
        P("sp", "tp"),
        P("sp", "tp"),
        P(None, "tp"),
        P("tp"),
        P("sp", None),
        P("sp", None),
        P(),
        P(),
        P(),
        P(None, "tp"),
        P(None, "tp"),
        P(),
        P(),
        P("tp"),
        P("tp", "sp"),
        P("tp", "sp"),
    )
    return jax.shard_map(
        on_device, mesh=mesh, in_specs=placed, out_specs=P(("sp", "tp"), None), check_vma=False
    )
```

```python
import functools

import jax
import jax.numpy as jnp
import numpy as np
from jax import lax
from jax.experimental import pallas as pl
from jax.experimental.pallas import tpu as pltpu
from jax.sharding import PartitionSpec as P

KEY_DIM = 128
VAL_DIM = 128
NOPE_DIM = 128
ROPE_DIM = 64
VHEAD_DIM = 128
ATT_QK = 192

norm_eps = 1e-06
rope_theta = 10000.0
MESH = pl.DeviceIdType.MESH
VMEM_LIMIT = 60 * 1024 * 1024
f32 = jnp.float32
bf16 = jnp.bfloat16


def rms_scale(values, gain_vec):
    mean_square = jnp.mean(values * values, axis=-1, keepdims=True)
    return values * lax.rsqrt(mean_square + norm_eps) * gain_vec


def greet(peers):
    barrier = pltpu.get_barrier_semaphore()
    for peer in peers:
        pl.semaphore_signal(barrier, inc=1, device_id=peer, device_id_type=MESH)
    pl.semaphore_wait(barrier, len(peers))


def line_and_pair(n):
    me = lax.axis_index("sp")
    lines = n // 2
    outer, inner = me // 2, lax.rem(me, 2)
    partner = {"sp": outer * 2 + 1 - inner}

    def line_peer(d):
        return {"sp": lax.rem(outer + d, lines) * 2 + inner}

    return me, lines, outer, inner, partner, line_peer


def project_kernel(n, count, x_ref, *refs):
    weights = refs[:count]
    outs = refs[count : 2 * count]
    rest = refs[2 * count :]
    x_recv = rest[0]
    w_recv = rest[1 : 1 + count]
    p_send = rest[1 + count : 1 + 2 * count]
    p_recv = rest[1 + 2 * count : 1 + 3 * count]
    own = rest[1 + 3 * count : 1 + 4 * count]
    xs, xr, ws, wr, ps, pr = rest[1 + 4 * count :]
    groups = n // 4
    me = lax.axis_index("sp")
    group, place = me // 4, lax.rem(me, 4)
    low, inner = place // 2, lax.rem(place, 2)
    places = (
        place,
        (1 - low) * 2 + inner,
        low * 2 + 1 - inner,
        (1 - low) * 2 + 1 - inner,
    )
    beside = {"sp": group * 4 + places[1]}
    partner = {"sp": group * 4 + places[2]}

    def far_peer(d):
        return {"sp": lax.rem(group + d, groups) * 4 + place}

    greet([beside, partner] + [far_peer(d) for d in range(1, groups)])

    def w_copy(c, k):
        return pltpu.make_async_remote_copy(
            src_ref=w_recv[c].at[0] if k == 2 else weights[c],
            dst_ref=w_recv[c].at[k],
            send_sem=ws.at[c, k],
            recv_sem=wr.at[c, k],
            device_id=beside if k == 0 else partner,
            device_id_type=MESH,
        )

    def x_copy(d):
        return pltpu.make_async_remote_copy(
            src_ref=x_ref.at[lax.rem(group + d, groups)],
            dst_ref=x_recv.at[d],
            send_sem=xs.at[d],
            recv_sem=xr.at[d],
            device_id=far_peer(d),
            device_id_type=MESH,
        )

    def p_copy(c, d):
        return pltpu.make_async_remote_copy(
            src_ref=p_send[c].at[d],
            dst_ref=p_recv[c].at[d],
            send_sem=ps.at[c, d],
            recv_sem=pr.at[c, d],
            device_id=far_peer(d),
            device_id_type=MESH,
        )

    w_copy(0, 0).start()
    w_copy(0, 1).start()
    for d in range(1, groups):
        x_copy(d).start()
    for c in range(1, count):
        w_copy(c, 0).start()
    for c in range(count):
        w_copy(c, 0).wait_recv()
        w_copy(c, 2).start()
        if c + 1 < count:
            w_copy(c + 1, 1).start()
    for c in range(count):
        w_copy(c, 1).wait_recv()
        w_copy(c, 2).wait_recv()

        def part(x):
            total = jnp.dot(x(places[0]), weights[c][...], preferred_element_type=f32)
            for k in range(3):
                total += jnp.dot(x(places[k + 1]), w_recv[c][k], preferred_element_type=f32)
            return total

        @pl.loop(1, groups)
        def _(d):
            if c == 0:
                x_copy(d).wait_recv()
            back = groups - d
            p_send[c][back] = part(lambda k: x_recv[d, k]).astype(bf16)
            p_copy(c, back).start()

        own[c][...] = part(lambda k: x_ref[group, k])
    for c in range(count):

        def add(d, total):
            p_copy(c, d).wait_recv()
            return total + p_recv[c][d].astype(f32)

        outs[c][...] = lax.fori_loop(1, groups, add, own[c][...]).astype(bf16)
    for d in range(1, groups):
        x_copy(d).wait_send()
    for c in range(count):
        for k in range(3):
            w_copy(c, k).wait_send()

        @pl.loop(1, groups)
        def _(d):
            p_copy(c, d).wait_send()


def project_all(n, x_split, weights):
    groups = n // 4
    rows, depth = x_split.shape[2:]
    count = len(weights)
    widths = [w.shape[1] for w in weights]
    vmem = pl.BlockSpec(memory_space=pltpu.VMEM)
    return pl.pallas_call(
        functools.partial(project_kernel, n, count),
        out_shape=[jax.ShapeDtypeStruct((rows, c), bf16) for c in widths],
        in_specs=[vmem] * (1 + count),
        out_specs=[vmem] * count,
        scratch_shapes=[pltpu.VMEM((groups, 4, rows, depth), bf16)]
        + [pltpu.VMEM((3, depth, c), bf16) for c in widths]
        + [pltpu.VMEM((groups, rows, c), bf16) for c in widths]
        + [pltpu.VMEM((groups, rows, c), bf16) for c in widths]
        + [pltpu.VMEM((rows, c), f32) for c in widths]
        + [
            pltpu.SemaphoreType.DMA((groups,)),
            pltpu.SemaphoreType.DMA((groups,)),
            pltpu.SemaphoreType.DMA((count, 3)),
            pltpu.SemaphoreType.DMA((count, 3)),
            pltpu.SemaphoreType.DMA((count, groups)),
            pltpu.SemaphoreType.DMA((count, groups)),
        ],
        compiler_params=pltpu.CompilerParams(
            collective_id=0, has_side_effects=True, vmem_limit_bytes=VMEM_LIMIT
        ),
    )(x_split, *weights)


def heads_peer(n, d):
    return {"tp": lax.rem(lax.axis_index("tp") + d, n)}


def mixer_kernel(n, heads_n, *refs):
    count = 5
    query_in, pair_in, ins = refs[0], refs[1], refs[2 : 2 + count]
    (
        fq_ref,
        fk_ref,
        bq_ref,
        bk_ref,
        v_ref,
        gate_ref,
        chain_gain_ref,
        query_latent_gain_ref,
        latent_gain_ref,
        query_up_ref,
        latent_up_ref,
        query_gain_ref,
        key_gain_ref,
        mixer_gain_ref,
        query_cos_ref,
        query_sin_ref,
        key_cos_ref,
        key_sin_ref,
        pick_key_ref,
        swap_key_ref,
        pick_plain_ref,
        pick_query_ref,
        swap_query_ref,
        out_ref,
    ) = refs[2 + count : 26 + count]
    rest = refs[26 + count :]
    query_out, pair_out, outs = rest[0], rest[1], rest[2 : 2 + count]
    numer, denom, send, recv, keep, s1, r1, s2, r2, hs1, hr1, hs2, hr2, ss, rs = rest[2 + count :]
    me, lines, outer, inner, partner, line_peer = line_and_pair(n)
    head = lax.axis_index("tp")
    head_lines = heads_n // 2
    head_outer, head_inner = head // 2, lax.rem(head, 2)
    head_partner = {"tp": head_outer * 2 + 1 - head_inner}

    def head_peer(d):
        return {"tp": lax.rem(head_outer + d, head_lines) * 2 + head_inner}

    greet(
        [partner]
        + [line_peer(d) for d in range(1, lines)]
        + [heads_peer(heads_n, d) for d in range(1, heads_n)]
    )
    src = (pair_in,) + tuple(ins)

    def slot(k, at):
        return pair_out.at[head, at] if k == 0 else outs[k - 1].at[at]

    def along(k, d):
        return pltpu.make_async_remote_copy(
            src_ref=src[k],
            dst_ref=slot(k, me),
            send_sem=s1.at[k, d],
            recv_sem=r1.at[k, d],
            device_id=line_peer(d),
            device_id_type=MESH,
        )

    def across(k, d):
        at = lax.rem(outer - d + lines, lines) * 2 + inner
        return pltpu.make_async_remote_copy(
            src_ref=src[k] if isinstance(d, int) and d == 0 else slot(k, at),
            dst_ref=slot(k, at),
            send_sem=s2.at[k, d],
            recv_sem=r2.at[k, d],
            device_id=partner,
            device_id_type=MESH,
        )

    def local(k):
        return pltpu.make_async_copy(src[k], slot(k, me), keep.at[k])

    def head_along(j, d):
        return pltpu.make_async_remote_copy(
            src_ref=query_in if j == 0 else pair_out.at[head],
            dst_ref=query_out.at[head] if j == 0 else pair_out.at[head],
            send_sem=hs1.at[j, d],
            recv_sem=hr1.at[j, d],
            device_id=head_peer(d),
            device_id_type=MESH,
        )

    def head_across(j, d):
        at = lax.rem(head_outer - d + head_lines, head_lines) * 2 + head_inner
        own = isinstance(d, int) and d == 0
        out = query_out if j == 0 else pair_out
        return pltpu.make_async_remote_copy(
            src_ref=query_in if j == 0 and own else out.at[at],
            dst_ref=out.at[at],
            send_sem=hs2.at[j, d],
            recv_sem=hr2.at[j, d],
            device_id=head_partner,
            device_id_type=MESH,
        )

    query_local = pltpu.make_async_copy(query_in, query_out.at[head], keep.at[1 + count])

    def needed(k, there):
        if k == 2:
            return there
        if k == 3:
            return jnp.logical_not(there)
        return None

    def maybe(condition, act):
        if condition is None:
            act()
        else:
            pl.when(condition)(act)

    def on_line(k, sending, act):
        @pl.loop(1, lines)
        def _(d):
            there = outer + d < lines if sending else outer >= d
            maybe(needed(k, there), lambda: act(d))

    for k in range(1 + count):
        on_line(k, True, lambda d: along(k, d).start())
        across(k, 0).start()
        local(k).start()
        if k == 0:
            for d in range(1, head_lines):
                head_along(0, d).start()
            head_across(0, 0).start()
            query_local.start()

    def pass_on(k):
        def act(d):
            along(k, d).wait_recv()
            across(k, d).start()

        on_line(k, False, act)

    pass_on(0)
    for d in range(1, head_lines):
        head_along(0, d).wait_recv()
        head_across(0, d).start()
    local(0).wait()
    across(0, 0).wait_recv()
    on_line(0, False, lambda d: across(0, d).wait_recv())
    for d in range(1, head_lines):
        head_along(1, d).start()
    head_across(1, 0).start()
    for k in range(1, count - 1):
        pass_on(k)

    rows, width = v_ref.shape
    chain_heads = width // KEY_DIM

    def lanes(h, size):
        return slice(h * size, (h + 1) * size)

    def against(a, b):
        return lax.dot_general(a, b, (((1,), (1,)), ((), ())), preferred_element_type=f32)

    row = lax.broadcasted_iota(jnp.int32, (rows, rows), 0)
    col = lax.broadcasted_iota(jnp.int32, (rows, rows), 1)
    within = []
    for h in range(chain_heads):
        at = lanes(h, KEY_DIM)
        both = jnp.where(row >= col, against(fq_ref[:, at], fk_ref[:, at]), 0.0) + jnp.where(
            row <= col, against(bq_ref[:, at], bk_ref[:, at]), 0.0
        )
        within.append(
            jnp.dot(both.astype(bf16), v_ref[:, lanes(h, VAL_DIM)], preferred_element_type=f32)
        )

    for d in range(1, head_lines):
        head_along(1, d).wait_recv()
        head_across(1, d).start()
    for k in (1, 2, 3):
        local(k).wait()
        across(k, 0).wait_recv()
        on_line(k, False, lambda d: across(k, d).wait_recv())

    log_ref, f_ref, b_ref = outs[0], outs[1], outs[2]

    def forward(i, state):
        return state * jnp.exp(log_ref[i, 0:1, :]) + f_ref[i].astype(f32)

    def backward(i, state):
        at = n - 1 - i
        return state * jnp.exp(log_ref[at, 1:2, :]) + b_ref[at].astype(f32)

    nothing = jnp.zeros(f_ref.shape[1:], f32)
    f_in = lax.fori_loop(0, me, forward, nothing).astype(bf16)
    b_in = lax.fori_loop(0, n - 1 - me, backward, nothing).astype(bf16)

    def normed(values, size):
        return lax.rsqrt(jnp.sum(values * values, axis=-1, keepdims=True) / size + norm_eps)

    chain_parts = []
    for h in range(chain_heads):
        at = lanes(h, KEY_DIM)
        total = (
            within[h] + against(fq_ref[:, at], f_in[:, at]) + against(bq_ref[:, at], b_in[:, at])
        )
        gate = gate_ref[:, lanes(h, VAL_DIM)].astype(f32)
        scaled = total * normed(total, VAL_DIM) * chain_gain_ref[:, lanes(h, VAL_DIM)]
        chain_parts.append((scaled * (gate * jax.nn.sigmoid(gate))).astype(bf16))
    chain_mixed = jnp.concatenate(chain_parts, axis=1)
    pass_on(4)

    query_local.wait()
    for j in range(head_lines):
        head_across(0, j).wait_recv()
    raws = [query_out[t].astype(f32) for t in range(heads_n)]
    q_cols = raws[0].shape[1]
    square = sum(jnp.sum(r * r, axis=-1, keepdims=True) for r in raws)
    scale = lax.rsqrt(square / (heads_n * q_cols) + norm_eps)
    attend_q = sum(
        jnp.dot(
            (raws[t] * scale * query_latent_gain_ref[t]).astype(bf16),
            query_up_ref[t],
            preferred_element_type=f32,
        )
        for t in range(heads_n)
    ).astype(bf16)
    heads = pick_plain_ref.shape[0]
    q_plain, q_turned = [], []
    for h in range(heads):
        plain = jnp.dot(attend_q, pick_plain_ref[h], preferred_element_type=f32)
        tail = jnp.dot(attend_q, pick_query_ref[h], preferred_element_type=f32)
        swapped = jnp.dot(attend_q, swap_query_ref[h], preferred_element_type=f32)
        square = jnp.sum(plain * plain, axis=-1, keepdims=True) + jnp.sum(
            tail * tail, axis=-1, keepdims=True
        )
        scale = lax.rsqrt(square / ATT_QK + norm_eps)
        q_plain.append((plain * scale * query_gain_ref[...]).astype(bf16))
        q_turned.append(
            ((tail * query_cos_ref[...] + swapped * query_sin_ref[...]) * scale).astype(bf16)
        )

    for d in range(head_lines):
        head_across(1, d).wait_recv()
    numer[...] = jnp.zeros_like(numer)
    denom[...] = jnp.zeros_like(denom)
    l_cols = latent_up_ref.shape[0] // heads_n

    def attend(at, carry):
        pieces = [pair_out[t, at] for t in range(heads_n)]
        wide = [p[:, :l_cols].astype(f32) for p in pieces]
        square = sum(jnp.sum(w * w, axis=-1, keepdims=True) for w in wide)
        scale = lax.rsqrt(square / (heads_n * l_cols) + norm_eps)
        latent = jnp.concatenate(
            [
                (wide[t] * scale * latent_gain_ref[:, lanes(t, l_cols)]).astype(bf16)
                for t in range(heads_n)
            ],
            axis=1,
        )
        pairs = jnp.dot(latent, latent_up_ref[...], preferred_element_type=f32).astype(bf16)
        tail = sum(
            jnp.dot(pieces[t], pick_key_ref[t], preferred_element_type=f32)
            for t in range(heads_n)
        )
        swapped = sum(
            jnp.dot(pieces[t], swap_key_ref[t], preferred_element_type=f32)
            for t in range(heads_n)
        )
        tail_square = jnp.sum(tail * tail, axis=-1, keepdims=True)
        turned = tail * key_cos_ref[at] + swapped * key_sin_ref[at]
        for h in range(heads):
            start = h * (NOPE_DIM + VHEAD_DIM)
            plain = pairs[:, start : start + NOPE_DIM].astype(f32)
            value = pairs[:, start + NOPE_DIM : start + NOPE_DIM + VHEAD_DIM]
            square = jnp.sum(plain * plain, axis=-1, keepdims=True) + tail_square
            scale = lax.rsqrt(square / ATT_QK + norm_eps)
            score = against(
                q_plain[h], (plain * scale * key_gain_ref[...]).astype(bf16)
            ) + against(q_turned[h], (turned * scale).astype(bf16))
            weight = jnp.exp(score * ATT_QK ** (-0.5))
            numer[h] += jnp.dot(weight.astype(bf16), value, preferred_element_type=f32)
            denom[h] += jnp.sum(weight, axis=-1, keepdims=True)
        return carry

    lax.fori_loop(0, n // 2, attend, 0)
    pass_on(5)
    lax.fori_loop(n // 2, n, attend, 0)
    attend_parts = []
    for h in range(heads):
        total = numer[h] / denom[h]
        gain = mixer_gain_ref[:, lanes(h, VHEAD_DIM)]
        attend_parts.append((total * normed(total, VHEAD_DIM) * gain).astype(bf16))
    attend_mixed = jnp.concatenate(attend_parts, axis=1)

    for k in (4, 5):
        local(k).wait()
        across(k, 0).wait_recv()
        on_line(k, False, lambda d: across(k, d).wait_recv())
    wc_ref, wa_ref = outs[3], outs[4]
    col_n = wc_ref.shape[2]
    part_rows = rows // heads_n
    for i in range(n):
        product = jnp.dot(chain_mixed, wc_ref[i], preferred_element_type=f32) + jnp.dot(
            attend_mixed, wa_ref[i], preferred_element_type=f32
        )
        for t in range(heads_n):
            send[t, :, lanes(i, col_n)] = product[lanes(t, part_rows)].astype(bf16)

    def sum_copy(d):
        return pltpu.make_async_remote_copy(
            src_ref=send.at[lax.rem(head + d, heads_n)],
            dst_ref=recv.at[d],
            send_sem=ss.at[d],
            recv_sem=rs.at[d],
            device_id=heads_peer(heads_n, d),
            device_id_type=MESH,
        )

    for d in range(1, heads_n):
        sum_copy(d).start()
    total = send[head].astype(f32)
    for d in range(1, heads_n):
        sum_copy(d).wait_recv()
        total = total + recv[d].astype(f32)
    out_ref[...] = total

    for d in range(1, heads_n):
        sum_copy(d).wait_send()
    for k in range(1 + count):
        across(k, 0).wait_send()
        on_line(k, True, lambda d: along(k, d).wait_send())
        on_line(k, False, lambda d: across(k, d).wait_send())
    for j in range(2):
        head_across(j, 0).wait_send()
        for d in range(1, head_lines):
            head_along(j, d).wait_send()
            head_across(j, d).wait_send()


def mix_all(n, heads_n, query, pair, blocks, others, heads):
    lines, head_lines = n // 2, heads_n // 2
    count = len(blocks)
    rows = query.shape[0]
    out_cols = n * blocks[-1].shape[1]
    vmem = pl.BlockSpec(memory_space=pltpu.VMEM)
    return pl.pallas_call(
        functools.partial(mixer_kernel, n, heads_n),
        out_shape=jax.ShapeDtypeStruct((rows // heads_n, out_cols), f32),
        in_specs=[vmem] * (2 + count + len(others)),
        out_specs=vmem,
        scratch_shapes=[
            pltpu.VMEM((heads_n,) + query.shape, query.dtype),
            pltpu.VMEM((heads_n, n) + pair.shape, pair.dtype),
        ]
        + [pltpu.VMEM((n,) + b.shape, b.dtype) for b in blocks]
        + [
            pltpu.VMEM((heads, rows, VHEAD_DIM), f32),
            pltpu.VMEM((heads, rows, 1), f32),
            pltpu.VMEM((heads_n, rows // heads_n, out_cols), bf16),
            pltpu.VMEM((heads_n, rows // heads_n, out_cols), bf16),
            pltpu.SemaphoreType.DMA((2 + count,)),
        ]
        + [pltpu.SemaphoreType.DMA((1 + count, lines))] * 4
        + [pltpu.SemaphoreType.DMA((2, head_lines))] * 4
        + [pltpu.SemaphoreType.DMA((heads_n,))] * 2,
        compiler_params=pltpu.CompilerParams(
            collective_id=1, has_side_effects=True, vmem_limit_bytes=VMEM_LIMIT
        ),
    )(query, pair, *blocks, *others)


def gate_parts(pre_gate, rate_row, seq_len):
    opening = rate_row / seq_len * jax.nn.sigmoid(-pre_gate.astype(f32))
    return (jnp.log1p(-opening), opening)


def on_device(
    tokens,
    input_gain,
    chain_query,
    forward_gate,
    backward_gate,
    chain_value,
    output_gate,
    forget_rate,
    chain_gain,
    query_down,
    latent_down,
    rotary_down,
    query_latent_gain,
    latent_gain,
    query_up,
    latent_up,
    query_head_gain,
    key_head_gain,
    mixer_gain,
    chain_out,
    attend_out,
):
    n_sp, n_tp = lax.axis_size("sp"), lax.axis_size("tp")
    sp, tp = lax.axis_index("sp"), lax.axis_index("tp")
    rows, depth = tokens.shape[0], chain_query.shape[0]
    seq_len = rows * n_sp
    q_cols = query_down.shape[1] // n_tp
    l_cols = latent_down.shape[1] // n_tp
    r_cols = ROPE_DIM // n_tp
    q_down = lax.dynamic_slice_in_dim(query_down, tp * q_cols, q_cols, 1)
    l_down = jnp.concatenate(
        [
            lax.dynamic_slice_in_dim(latent_down, tp * l_cols, l_cols, 1),
            lax.dynamic_slice(rotary_down, (sp * depth, tp * r_cols), (depth, r_cols)),
        ],
        axis=1,
    )
    normed = rms_scale(tokens.astype(f32), input_gain).astype(bf16)
    x_split = normed.reshape(rows, n_sp // 4, 4, depth).transpose(1, 2, 0, 3)
    raw_q, raw_l, q_rows, fwd_logit, bwd_logit, v_rows, gate_logit = project_all(
        n_sp,
        x_split,
        (q_down, l_down, chain_query, forward_gate, backward_gate, chain_value, output_gate),
    )

    f_log, f_key = gate_parts(fwd_logit, forget_rate[0], seq_len)
    b_log, b_key = gate_parts(bwd_logit, forget_rate[1], seq_len)
    width = f_log.shape[1]
    chain_heads = width // KEY_DIM
    lower = jnp.tril(jnp.ones((rows, rows), f32))
    f_cum = jnp.dot(lower, f_log, precision=lax.Precision.HIGHEST)
    b_cum = jnp.dot(lower.T, b_log, precision=lax.Precision.HIGHEST)
    q_wide = q_rows.astype(f32)

    f_q, f_k = (q_wide * jnp.exp(f_cum)).astype(bf16), (f_key * jnp.exp(-f_cum)).astype(bf16)
    b_q, b_k = (q_wide * jnp.exp(b_cum)).astype(bf16), (b_key * jnp.exp(-b_cum)).astype(bf16)
    logs = jnp.stack([f_cum[-1], b_cum[0]])

    def digest(keys, log):
        parts = [
            lax.dot_general(
                v_rows[:, h * VAL_DIM : (h + 1) * VAL_DIM],
                keys[:, h * KEY_DIM : (h + 1) * KEY_DIM],
                (((0,), (0,)), ((), ())),
                preferred_element_type=f32,
            )
            for h in range(chain_heads)
        ]
        return (jnp.concatenate(parts, axis=1) * jnp.exp(log)).astype(bf16)

    heads = query_up.shape[1] // ATT_QK
    half = ROPE_DIM // 2
    inverse = rope_theta ** (-jnp.arange(0, ROPE_DIM, 2).astype(f32) / ROPE_DIM)
    angles = jnp.arange(seq_len, dtype=jnp.int32).astype(f32)[:, None] * inverse
    cosine = jnp.tile(jnp.cos(angles), (1, 2))
    sine = jnp.tile(jnp.sin(angles), (1, 2))

    def tables(gain, cos_rows, sin_rows):
        tail = gain[NOPE_DIM:]
        return cos_rows * tail, sin_rows * jnp.roll(tail, half)

    own_rows = functools.partial(
        lax.dynamic_slice_in_dim, start_index=sp * rows, slice_size=rows, axis=0
    )
    query_tables = tables(query_head_gain, own_rows(cosine), own_rows(sine))
    key_tables = [
        t.reshape(n_sp, rows, ROPE_DIM) for t in tables(key_head_gain, cosine, sine)
    ]
    swap = np.zeros((ROPE_DIM, ROPE_DIM), np.float32)
    for j in range(half):
        swap[half + j, j] = -1.0
        swap[j, half + j] = 1.0
    pick_key = np.zeros((n_tp, l_cols + r_cols, ROPE_DIM), np.float32)
    for t in range(n_tp):
        for j in range(r_cols):
            pick_key[t, l_cols + j, t * r_cols + j] = 1.0
    pick_plain = np.zeros((heads, heads * ATT_QK, NOPE_DIM), np.float32)
    pick_query = np.zeros((heads, heads * ATT_QK, ROPE_DIM), np.float32)
    for h in range(heads):
        for j in range(NOPE_DIM):
            pick_plain[h, h * ATT_QK + j, j] = 1.0
        for j in range(ROPE_DIM):
            pick_query[h, h * ATT_QK + NOPE_DIM + j, j] = 1.0
    picks = [
        jnp.asarray(p, bf16)
        for p in (pick_key, pick_key @ swap, pick_plain, pick_query, pick_query @ swap)
    ]
    return mix_all(
        n_sp,
        n_tp,
        raw_q,
        raw_l,
        (logs, digest(f_k, logs[0]), digest(b_k, logs[1]), chain_out, attend_out),
        (
            f_q,
            f_k,
            b_q,
            b_k,
            v_rows,
            gate_logit,
            chain_gain[None],
            query_latent_gain.reshape(n_tp, 1, q_cols),
            latent_gain[None],
            query_up.reshape(n_tp, q_cols, -1),
            latent_up,
            query_head_gain[None, :NOPE_DIM],
            key_head_gain[None, :NOPE_DIM],
            mixer_gain[None],
            *query_tables,
            *key_tables,
            *picks,
        ),
        heads,
    )


def solution(mesh):
    placed = (
        P("sp", None),
        P(),
        P("sp", "tp"),
        P("sp", "tp"),
        P("sp", "tp"),
        P("sp", "tp"),
        P("sp", "tp"),
        P(None, "tp"),
        P("tp"),
        P("sp", None),
        P("sp", None),
        P(),
        P(),
        P(),
        P(None, "tp"),
        P(None, "tp"),
        P(),
        P(),
        P("tp"),
        P("tp", "sp"),
        P("tp", "sp"),
    )
    return jax.shard_map(
        on_device, mesh=mesh, in_specs=placed, out_specs=P(("sp", "tp"), None), check_vma=False
    )
```

```python
import functools

import jax
import jax.numpy as jnp
import numpy as np
from jax import lax
from jax.experimental import pallas as pl
from jax.experimental.pallas import tpu as pltpu
from jax.sharding import PartitionSpec as P

KEY_DIM = 128
VAL_DIM = 128
NOPE_DIM = 128
ROPE_DIM = 64
VHEAD_DIM = 128
ATT_QK = 192

norm_eps = 1e-06
rope_theta = 10000.0
MESH = pl.DeviceIdType.MESH
VMEM_LIMIT = 60 * 1024 * 1024
f32 = jnp.float32
bf16 = jnp.bfloat16


def greet(peers):
    barrier = pltpu.get_barrier_semaphore()
    for peer in peers:
        pl.semaphore_signal(barrier, inc=1, device_id=peer, device_id_type=MESH)
    pl.semaphore_wait(barrier, len(peers))


def line_and_pair(n):
    me = lax.axis_index("sp")
    lines = n // 2
    outer, inner = me // 2, lax.rem(me, 2)
    partner = {"sp": outer * 2 + 1 - inner}

    def line_peer(d):
        return {"sp": lax.rem(outer + d, lines) * 2 + inner}

    return me, lines, outer, inner, partner, line_peer


def project_kernel(n, count, *refs):
    tokens_ref, gain_ref, rate_ref = refs[:3]
    weights = refs[3 : 3 + count]
    (
        v_ref,
        gate_ref,
        ql_ref,
        ll_ref,
        fq_ref,
        fk_ref,
        bq_ref,
        bk_ref,
        log_ref,
        f_state_ref,
        b_state_ref,
    ) = refs[3 + count : 14 + count]
    rest = refs[14 + count :]
    x_ref, x_recv = rest[0], rest[1]
    w_recv = rest[2 : 2 + count]
    p_send = rest[2 + count : 2 + 2 * count]
    p_recv = rest[2 + 2 * count : 2 + 3 * count]
    own = rest[2 + 3 * count : 2 + 4 * count]
    xs, xr, ws, wr, ps, pr = rest[2 + 4 * count :]
    groups = n // 4
    me = lax.axis_index("sp")
    group, place = me // 4, lax.rem(me, 4)
    low, inner = place // 2, lax.rem(place, 2)
    places = (
        place,
        (1 - low) * 2 + inner,
        low * 2 + 1 - inner,
        (1 - low) * 2 + 1 - inner,
    )
    beside = {"sp": group * 4 + places[1]}
    partner = {"sp": group * 4 + places[2]}

    def far_peer(d):
        return {"sp": lax.rem(group + d, groups) * 4 + place}

    greet([beside, partner] + [far_peer(d) for d in range(1, groups)])

    def w_copy(c, k):
        return pltpu.make_async_remote_copy(
            src_ref=w_recv[c].at[0] if k == 2 else weights[c],
            dst_ref=w_recv[c].at[k],
            send_sem=ws.at[c, k],
            recv_sem=wr.at[c, k],
            device_id=beside if k == 0 else partner,
            device_id_type=MESH,
        )

    def x_copy(d):
        return pltpu.make_async_remote_copy(
            src_ref=x_ref.at[lax.rem(group + d, groups)],
            dst_ref=x_recv.at[d],
            send_sem=xs.at[d],
            recv_sem=xr.at[d],
            device_id=far_peer(d),
            device_id_type=MESH,
        )

    def p_copy(c, d):
        return pltpu.make_async_remote_copy(
            src_ref=p_send[c].at[d],
            dst_ref=p_recv[c].at[d],
            send_sem=ps.at[c, d],
            recv_sem=pr.at[c, d],
            device_id=far_peer(d),
            device_id_type=MESH,
        )

    w_copy(0, 0).start()
    w_copy(0, 1).start()
    wide = tokens_ref[...].astype(f32)
    scale = lax.rsqrt(jnp.mean(wide * wide, axis=-1, keepdims=True) + norm_eps)
    normed = (wide * scale * gain_ref[...]).astype(bf16)
    rows, depth = x_ref.shape[2:]
    for g in range(groups):
        for k in range(4):
            first = (g * 4 + k) * depth
            x_ref[g, k] = normed[:, first : first + depth]
    for d in range(1, groups):
        x_copy(d).start()
    for c in range(1, count):
        w_copy(c, 0).start()
    for c in range(count):
        w_copy(c, 0).wait_recv()
        w_copy(c, 2).start()
        if c + 1 < count:
            w_copy(c + 1, 1).start()
    def finished(c):
        def add(d, total):
            p_copy(c, d).wait_recv()
            return total + p_recv[c][d].astype(f32)

        return lax.fori_loop(1, groups, add, own[c][...]).astype(bf16)

    def recurrence():
        value = finished(0)
        v_ref[...] = value
        row = lax.broadcasted_iota(jnp.int32, (rows, rows), 0)
        col = lax.broadcasted_iota(jnp.int32, (rows, rows), 1)

        def direction(c, mask, last):
            rate = rate_ref[c - 1 : c, :] / (rows * n)
            key = rate * jax.nn.sigmoid(-finished(c).astype(f32))
            total = jnp.dot(
                jnp.where(mask, 1.0, 0.0),
                jnp.log1p(-key),
                precision=lax.Precision.HIGHEST,
                preferred_element_type=f32,
            )
            full = total[last : last + 1, :]
            key = (key * jnp.exp(-total)).astype(bf16)
            state = jnp.concatenate(
                [
                    lax.dot_general(
                        value[:, h * VAL_DIM : (h + 1) * VAL_DIM],
                        key[:, h * KEY_DIM : (h + 1) * KEY_DIM],
                        (((0,), (0,)), ((), ())),
                        preferred_element_type=f32,
                    )
                    for h in range(value.shape[1] // VAL_DIM)
                ],
                axis=1,
            )
            log_ref[c - 1 : c, :] = full
            return key, total, (state * jnp.exp(full)).astype(bf16)

        fk_ref[...], f_total, f_state_ref[...] = direction(1, row >= col, rows - 1)
        bk_ref[...], b_total, b_state_ref[...] = direction(2, row <= col, 0)
        query = finished(3).astype(f32)
        fq_ref[...] = (query * jnp.exp(f_total)).astype(bf16)
        bq_ref[...] = (query * jnp.exp(b_total)).astype(bf16)

    for c in range(count):
        w_copy(c, 1).wait_recv()
        w_copy(c, 2).wait_recv()

        def part(x):
            total = jnp.dot(x(places[0]), weights[c][...], preferred_element_type=f32)
            for k in range(3):
                total += jnp.dot(x(places[k + 1]), w_recv[c][k], preferred_element_type=f32)
            return total

        @pl.loop(1, groups)
        def _(d):
            if c == 0:
                x_copy(d).wait_recv()
            back = groups - d
            p_send[c][back] = part(lambda k: x_recv[d, k]).astype(bf16)
            p_copy(c, back).start()

        own[c][...] = part(lambda k: x_ref[group, k])
        if c == count - 2:
            recurrence()
    gate_ref[...] = finished(4)
    ql_ref[...] = finished(5)
    ll_ref[...] = finished(6)
    for d in range(1, groups):
        x_copy(d).wait_send()
    for c in range(count):
        for k in range(3):
            w_copy(c, k).wait_send()

        @pl.loop(1, groups)
        def _(d):
            p_copy(c, d).wait_send()


def project_all(n, tokens, gain, rates, weights):
    groups = n // 4
    rows, depth = tokens.shape[0], weights[0].shape[0]
    count = len(weights)
    widths = [w.shape[1] for w in weights]
    width = widths[0]
    wide = jax.ShapeDtypeStruct((rows, width), bf16)
    state = jax.ShapeDtypeStruct((VAL_DIM, width), bf16)
    vmem = pl.BlockSpec(memory_space=pltpu.VMEM)
    return pl.pallas_call(
        functools.partial(project_kernel, n, count),
        out_shape=[jax.ShapeDtypeStruct((rows, widths[c]), bf16) for c in (0, 4, 5, 6)]
        + [wide] * 4
        + [jax.ShapeDtypeStruct((2, width), f32), state, state],
        in_specs=[vmem] * (3 + count),
        out_specs=[vmem] * 11,
        scratch_shapes=[pltpu.VMEM((groups, 4, rows, depth), bf16)] * 2
        + [pltpu.VMEM((3, depth, c), bf16) for c in widths]
        + [pltpu.VMEM((groups, rows, c), bf16) for c in widths]
        + [pltpu.VMEM((groups, rows, c), bf16) for c in widths]
        + [pltpu.VMEM((rows, c), f32) for c in widths]
        + [
            pltpu.SemaphoreType.DMA((groups,)),
            pltpu.SemaphoreType.DMA((groups,)),
            pltpu.SemaphoreType.DMA((count, 3)),
            pltpu.SemaphoreType.DMA((count, 3)),
            pltpu.SemaphoreType.DMA((count, groups)),
            pltpu.SemaphoreType.DMA((count, groups)),
        ],
        compiler_params=pltpu.CompilerParams(
            collective_id=0, has_side_effects=True, vmem_limit_bytes=VMEM_LIMIT
        ),
    )(tokens, gain, rates, *weights)


def heads_peer(n, d):
    return {"tp": lax.rem(lax.axis_index("tp") + d, n)}


def mixer_kernel(n, heads_n, *refs):
    count = 5
    query_in, pair_in, ins = refs[0], refs[1], refs[2 : 2 + count]
    (
        fq_ref,
        fk_ref,
        bq_ref,
        bk_ref,
        v_ref,
        gate_ref,
        chain_gain_ref,
        query_latent_gain_ref,
        latent_gain_ref,
        query_up_ref,
        latent_up_ref,
        query_gain_ref,
        key_gain_ref,
        mixer_gain_ref,
        query_tail_ref,
        key_tail_ref,
        cos_ref,
        sin_ref,
        pick_key_ref,
        swap_key_ref,
        pick_plain_ref,
        pick_query_ref,
        swap_query_ref,
        out_ref,
    ) = refs[2 + count : 26 + count]
    rest = refs[26 + count :]
    query_out, pair_out, outs = rest[0], rest[1], rest[2 : 2 + count]
    numer, denom, send, recv, keep, s1, r1, s2, r2, hs1, hr1, hs2, hr2, ss, rs = rest[2 + count :]
    me, lines, outer, inner, partner, line_peer = line_and_pair(n)
    head = lax.axis_index("tp")
    head_lines = heads_n // 2
    head_outer, head_inner = head // 2, lax.rem(head, 2)
    head_partner = {"tp": head_outer * 2 + 1 - head_inner}

    def head_peer(d):
        return {"tp": lax.rem(head_outer + d, head_lines) * 2 + head_inner}

    greet(
        [partner]
        + [line_peer(d) for d in range(1, lines)]
        + [heads_peer(heads_n, d) for d in range(1, heads_n)]
    )
    src = (pair_in,) + tuple(ins)

    def slot(k, at):
        return pair_out.at[head, at] if k == 0 else outs[k - 1].at[at]

    def along(k, d):
        return pltpu.make_async_remote_copy(
            src_ref=src[k],
            dst_ref=slot(k, me),
            send_sem=s1.at[k, d],
            recv_sem=r1.at[k, d],
            device_id=line_peer(d),
            device_id_type=MESH,
        )

    def across(k, d):
        at = lax.rem(outer - d + lines, lines) * 2 + inner
        return pltpu.make_async_remote_copy(
            src_ref=src[k] if isinstance(d, int) and d == 0 else slot(k, at),
            dst_ref=slot(k, at),
            send_sem=s2.at[k, d],
            recv_sem=r2.at[k, d],
            device_id=partner,
            device_id_type=MESH,
        )

    def local(k):
        return pltpu.make_async_copy(src[k], slot(k, me), keep.at[k])

    def head_along(j, d):
        return pltpu.make_async_remote_copy(
            src_ref=query_in if j == 0 else pair_out.at[head],
            dst_ref=query_out.at[head] if j == 0 else pair_out.at[head],
            send_sem=hs1.at[j, d],
            recv_sem=hr1.at[j, d],
            device_id=head_peer(d),
            device_id_type=MESH,
        )

    def head_across(j, d):
        at = lax.rem(head_outer - d + head_lines, head_lines) * 2 + head_inner
        own = isinstance(d, int) and d == 0
        out = query_out if j == 0 else pair_out
        return pltpu.make_async_remote_copy(
            src_ref=query_in if j == 0 and own else out.at[at],
            dst_ref=out.at[at],
            send_sem=hs2.at[j, d],
            recv_sem=hr2.at[j, d],
            device_id=head_partner,
            device_id_type=MESH,
        )

    query_local = pltpu.make_async_copy(query_in, query_out.at[head], keep.at[1 + count])

    def needed(k, there):
        if k == 2:
            return there
        if k == 3:
            return jnp.logical_not(there)
        return None

    def maybe(condition, act):
        if condition is None:
            act()
        else:
            pl.when(condition)(act)

    def on_line(k, sending, act):
        @pl.loop(1, lines)
        def _(d):
            there = outer + d < lines if sending else outer >= d
            maybe(needed(k, there), lambda: act(d))

    for k in range(1 + count):
        on_line(k, True, lambda d: along(k, d).start())
        across(k, 0).start()
        local(k).start()
        if k == 0:
            for d in range(1, head_lines):
                head_along(0, d).start()
            head_across(0, 0).start()
            query_local.start()

    def pass_on(k):
        def act(d):
            along(k, d).wait_recv()
            across(k, d).start()

        on_line(k, False, act)

    pass_on(0)
    for d in range(1, head_lines):
        head_along(0, d).wait_recv()
        head_across(0, d).start()
    local(0).wait()
    across(0, 0).wait_recv()
    on_line(0, False, lambda d: across(0, d).wait_recv())
    for d in range(1, head_lines):
        head_along(1, d).start()
    head_across(1, 0).start()
    for k in range(1, count - 1):
        pass_on(k)

    rows, width = v_ref.shape
    chain_heads = width // KEY_DIM

    def lanes(h, size):
        return slice(h * size, (h + 1) * size)

    def against(a, b):
        return lax.dot_general(a, b, (((1,), (1,)), ((), ())), preferred_element_type=f32)

    row = lax.broadcasted_iota(jnp.int32, (rows, rows), 0)
    col = lax.broadcasted_iota(jnp.int32, (rows, rows), 1)
    within = []
    for h in range(chain_heads):
        at = lanes(h, KEY_DIM)
        both = jnp.where(row >= col, against(fq_ref[:, at], fk_ref[:, at]), 0.0) + jnp.where(
            row <= col, against(bq_ref[:, at], bk_ref[:, at]), 0.0
        )
        within.append(
            jnp.dot(both.astype(bf16), v_ref[:, lanes(h, VAL_DIM)], preferred_element_type=f32)
        )

    for d in range(1, head_lines):
        head_along(1, d).wait_recv()
        head_across(1, d).start()
    for k in (1, 2, 3):
        local(k).wait()
        across(k, 0).wait_recv()
        on_line(k, False, lambda d: across(k, d).wait_recv())

    log_ref, f_ref, b_ref = outs[0], outs[1], outs[2]

    def forward(i, state):
        return state * jnp.exp(log_ref[i, 0:1, :]) + f_ref[i].astype(f32)

    def backward(i, state):
        at = n - 1 - i
        return state * jnp.exp(log_ref[at, 1:2, :]) + b_ref[at].astype(f32)

    nothing = jnp.zeros(f_ref.shape[1:], f32)
    f_in = lax.fori_loop(0, me, forward, nothing).astype(bf16)
    b_in = lax.fori_loop(0, n - 1 - me, backward, nothing).astype(bf16)

    def normed(values, size):
        return lax.rsqrt(jnp.sum(values * values, axis=-1, keepdims=True) / size + norm_eps)

    chain_parts = []
    for h in range(chain_heads):
        at = lanes(h, KEY_DIM)
        total = (
            within[h] + against(fq_ref[:, at], f_in[:, at]) + against(bq_ref[:, at], b_in[:, at])
        )
        gate = gate_ref[:, lanes(h, VAL_DIM)].astype(f32)
        scaled = total * normed(total, VAL_DIM) * chain_gain_ref[:, lanes(h, VAL_DIM)]
        chain_parts.append((scaled * (gate * jax.nn.sigmoid(gate))).astype(bf16))
    chain_mixed = jnp.concatenate(chain_parts, axis=1)
    pass_on(4)

    query_local.wait()
    for j in range(head_lines):
        head_across(0, j).wait_recv()
    raws = [query_out[t].astype(f32) for t in range(heads_n)]
    q_cols = raws[0].shape[1]
    square = sum(jnp.sum(r * r, axis=-1, keepdims=True) for r in raws)
    scale = lax.rsqrt(square / (heads_n * q_cols) + norm_eps)
    attend_q = sum(
        jnp.dot(
            (raws[t] * scale * query_latent_gain_ref[t]).astype(bf16),
            query_up_ref[lanes(t, q_cols), :],
            preferred_element_type=f32,
        )
        for t in range(heads_n)
    ).astype(bf16)
    heads = pick_plain_ref.shape[0]
    query_cos = cos_ref[me] * query_tail_ref[0:1, :]
    query_sin = sin_ref[me] * query_tail_ref[1:2, :]
    q_plain, q_turned = [], []
    for h in range(heads):
        plain = jnp.dot(attend_q, pick_plain_ref[h], preferred_element_type=f32)
        tail = jnp.dot(attend_q, pick_query_ref[h], preferred_element_type=f32)
        swapped = jnp.dot(attend_q, swap_query_ref[h], preferred_element_type=f32)
        square = jnp.sum(plain * plain, axis=-1, keepdims=True) + jnp.sum(
            tail * tail, axis=-1, keepdims=True
        )
        scale = lax.rsqrt(square / ATT_QK + norm_eps)
        q_plain.append((plain * scale * query_gain_ref[...]).astype(bf16))
        q_turned.append(
            ((tail * query_cos + swapped * query_sin) * scale).astype(bf16)
        )

    for d in range(head_lines):
        head_across(1, d).wait_recv()
    numer[...] = jnp.zeros_like(numer)
    denom[...] = jnp.zeros_like(denom)
    l_cols = latent_up_ref.shape[0] // heads_n

    def attend(at, carry):
        pieces = [pair_out[t, at] for t in range(heads_n)]
        wide = [p[:, :l_cols].astype(f32) for p in pieces]
        square = sum(jnp.sum(w * w, axis=-1, keepdims=True) for w in wide)
        scale = lax.rsqrt(square / (heads_n * l_cols) + norm_eps)
        latent = jnp.concatenate(
            [
                (wide[t] * scale * latent_gain_ref[:, lanes(t, l_cols)]).astype(bf16)
                for t in range(heads_n)
            ],
            axis=1,
        )
        pairs = jnp.dot(latent, latent_up_ref[...], preferred_element_type=f32).astype(bf16)
        tail = sum(
            jnp.dot(pieces[t], pick_key_ref[t], preferred_element_type=f32)
            for t in range(heads_n)
        )
        swapped = sum(
            jnp.dot(pieces[t], swap_key_ref[t], preferred_element_type=f32)
            for t in range(heads_n)
        )
        tail_square = jnp.sum(tail * tail, axis=-1, keepdims=True)
        turned = (tail * key_tail_ref[0:1, :]) * cos_ref[at] + (
            swapped * key_tail_ref[1:2, :]
        ) * sin_ref[at]
        for h in range(heads):
            start = h * (NOPE_DIM + VHEAD_DIM)
            plain = pairs[:, start : start + NOPE_DIM].astype(f32)
            value = pairs[:, start + NOPE_DIM : start + NOPE_DIM + VHEAD_DIM]
            square = jnp.sum(plain * plain, axis=-1, keepdims=True) + tail_square
            scale = lax.rsqrt(square / ATT_QK + norm_eps)
            score = against(
                q_plain[h], (plain * scale * key_gain_ref[...]).astype(bf16)
            ) + against(q_turned[h], (turned * scale).astype(bf16))
            weight = jnp.exp(score * ATT_QK ** (-0.5))
            numer[h] += jnp.dot(weight.astype(bf16), value, preferred_element_type=f32)
            denom[h] += jnp.sum(weight, axis=-1, keepdims=True)
        return carry

    lax.fori_loop(0, n // 2, attend, 0)
    pass_on(5)
    lax.fori_loop(n // 2, n, attend, 0)
    attend_parts = []
    for h in range(heads):
        total = numer[h] / denom[h]
        gain = mixer_gain_ref[:, lanes(h, VHEAD_DIM)]
        attend_parts.append((total * normed(total, VHEAD_DIM) * gain).astype(bf16))
    attend_mixed = jnp.concatenate(attend_parts, axis=1)

    for k in (4, 5):
        local(k).wait()
        across(k, 0).wait_recv()
        on_line(k, False, lambda d: across(k, d).wait_recv())
    wc_ref, wa_ref = outs[3], outs[4]
    col_n = wc_ref.shape[2]
    part_rows = rows // heads_n
    for i in range(n):
        product = jnp.dot(chain_mixed, wc_ref[i], preferred_element_type=f32) + jnp.dot(
            attend_mixed, wa_ref[i], preferred_element_type=f32
        )
        for t in range(heads_n):
            send[t, :, lanes(i, col_n)] = product[lanes(t, part_rows)].astype(bf16)

    def sum_copy(d):
        return pltpu.make_async_remote_copy(
            src_ref=send.at[lax.rem(head + d, heads_n)],
            dst_ref=recv.at[d],
            send_sem=ss.at[d],
            recv_sem=rs.at[d],
            device_id=heads_peer(heads_n, d),
            device_id_type=MESH,
        )

    for d in range(1, heads_n):
        sum_copy(d).start()
    total = send[head].astype(f32)
    for d in range(1, heads_n):
        sum_copy(d).wait_recv()
        total = total + recv[d].astype(f32)
    out_ref[...] = total

    for d in range(1, heads_n):
        sum_copy(d).wait_send()
    for k in range(1 + count):
        across(k, 0).wait_send()
        on_line(k, True, lambda d: along(k, d).wait_send())
        on_line(k, False, lambda d: across(k, d).wait_send())
    for j in range(2):
        head_across(j, 0).wait_send()
        for d in range(1, head_lines):
            head_along(j, d).wait_send()
            head_across(j, d).wait_send()


def mix_all(n, heads_n, query, pair, blocks, others, heads):
    lines, head_lines = n // 2, heads_n // 2
    count = len(blocks)
    rows = query.shape[0]
    out_cols = n * blocks[-1].shape[1]
    vmem = pl.BlockSpec(memory_space=pltpu.VMEM)
    return pl.pallas_call(
        functools.partial(mixer_kernel, n, heads_n),
        out_shape=jax.ShapeDtypeStruct((rows // heads_n, out_cols), f32),
        in_specs=[vmem] * (2 + count + len(others)),
        out_specs=vmem,
        scratch_shapes=[
            pltpu.VMEM((heads_n,) + query.shape, query.dtype),
            pltpu.VMEM((heads_n, n) + pair.shape, pair.dtype),
        ]
        + [pltpu.VMEM((n,) + b.shape, b.dtype) for b in blocks]
        + [
            pltpu.VMEM((heads, rows, VHEAD_DIM), f32),
            pltpu.VMEM((heads, rows, 1), f32),
            pltpu.VMEM((heads_n, rows // heads_n, out_cols), bf16),
            pltpu.VMEM((heads_n, rows // heads_n, out_cols), bf16),
            pltpu.SemaphoreType.DMA((2 + count,)),
        ]
        + [pltpu.SemaphoreType.DMA((1 + count, lines))] * 4
        + [pltpu.SemaphoreType.DMA((2, head_lines))] * 4
        + [pltpu.SemaphoreType.DMA((heads_n,))] * 2,
        compiler_params=pltpu.CompilerParams(
            collective_id=1, has_side_effects=True, vmem_limit_bytes=VMEM_LIMIT
        ),
    )(query, pair, *blocks, *others)


def on_device(
    tokens,
    input_gain,
    chain_query,
    forward_gate,
    backward_gate,
    chain_value,
    output_gate,
    forget_rate,
    chain_gain,
    query_down,
    latent_down,
    rotary_down,
    query_latent_gain,
    latent_gain,
    query_up,
    latent_up,
    query_head_gain,
    key_head_gain,
    mixer_gain,
    chain_out,
    attend_out,
):
    n_sp, n_tp = lax.axis_size("sp"), lax.axis_size("tp")
    sp, tp = lax.axis_index("sp"), lax.axis_index("tp")
    rows, depth = tokens.shape[0], chain_query.shape[0]
    seq_len = rows * n_sp
    q_cols = query_down.shape[1] // n_tp
    l_cols = latent_down.shape[1] // n_tp
    r_cols = ROPE_DIM // n_tp
    q_down = lax.dynamic_slice_in_dim(query_down, tp * q_cols, q_cols, 1)
    l_down = jnp.concatenate(
        [
            lax.dynamic_slice_in_dim(latent_down, tp * l_cols, l_cols, 1),
            lax.dynamic_slice(rotary_down, (sp * depth, tp * r_cols), (depth, r_cols)),
        ],
        axis=1,
    )
    (v_rows, gate_logit, raw_q, raw_l, f_q, f_k, b_q, b_k, logs, f_state, b_state) = project_all(
        n_sp,
        tokens,
        input_gain[None],
        forget_rate,
        (chain_value, forward_gate, backward_gate, chain_query, output_gate, q_down, l_down),
    )

    heads = query_up.shape[1] // ATT_QK
    half = ROPE_DIM // 2
    inverse = rope_theta ** (-np.arange(0, ROPE_DIM, 2).astype(np.float32) / ROPE_DIM)
    angles = np.arange(seq_len, dtype=np.float32)[:, None] * inverse.astype(np.float32)
    cosine, sine = (
        jnp.asarray(np.tile(turn(angles), (1, 2)).reshape(n_sp, rows, ROPE_DIM), f32)
        for turn in (np.cos, np.sin)
    )

    def tails(gain):
        tail = gain[NOPE_DIM:]
        return jnp.stack([tail, jnp.roll(tail, half)])

    swap = np.zeros((ROPE_DIM, ROPE_DIM), np.float32)
    for j in range(half):
        swap[half + j, j] = -1.0
        swap[j, half + j] = 1.0
    pick_key = np.zeros((n_tp, l_cols + r_cols, ROPE_DIM), np.float32)
    for t in range(n_tp):
        for j in range(r_cols):
            pick_key[t, l_cols + j, t * r_cols + j] = 1.0
    pick_plain = np.zeros((heads, heads * ATT_QK, NOPE_DIM), np.float32)
    pick_query = np.zeros((heads, heads * ATT_QK, ROPE_DIM), np.float32)
    for h in range(heads):
        for j in range(NOPE_DIM):
            pick_plain[h, h * ATT_QK + j, j] = 1.0
        for j in range(ROPE_DIM):
            pick_query[h, h * ATT_QK + NOPE_DIM + j, j] = 1.0
    picks = [
        jnp.asarray(p, bf16)
        for p in (pick_key, pick_key @ swap, pick_plain, pick_query, pick_query @ swap)
    ]
    return mix_all(
        n_sp,
        n_tp,
        raw_q,
        raw_l,
        (logs, f_state, b_state, chain_out, attend_out),
        (
            f_q,
            f_k,
            b_q,
            b_k,
            v_rows,
            gate_logit,
            chain_gain[None],
            query_latent_gain.reshape(n_tp, 1, q_cols),
            latent_gain[None],
            query_up,
            latent_up,
            query_head_gain[None, :NOPE_DIM],
            key_head_gain[None, :NOPE_DIM],
            mixer_gain[None],
            tails(query_head_gain),
            tails(key_head_gain),
            cosine,
            sine,
            *picks,
        ),
        heads,
    )


def solution(mesh):
    placed = (
        P("sp", None),
        P(),
        P("sp", "tp"),
        P("sp", "tp"),
        P("sp", "tp"),
        P("sp", "tp"),
        P("sp", "tp"),
        P(None, "tp"),
        P("tp"),
        P("sp", None),
        P("sp", None),
        P(),
        P(),
        P(),
        P(None, "tp"),
        P(None, "tp"),
        P(),
        P(),
        P("tp"),
        P("tp", "sp"),
        P("tp", "sp"),
    )
    return jax.shard_map(
        on_device, mesh=mesh, in_specs=placed, out_specs=P(("sp", "tp"), None), check_vma=False
    )
```

```python
import functools

import jax
import jax.numpy as jnp
import numpy as np
from jax import lax
from jax.experimental import pallas as pl
from jax.experimental.pallas import tpu as pltpu
from jax.sharding import PartitionSpec as P

KEY_DIM = 128
VAL_DIM = 128
NOPE_DIM = 128
ROPE_DIM = 64
VHEAD_DIM = 128
ATT_QK = 192

norm_eps = 1e-06
rope_theta = 10000.0
MESH = pl.DeviceIdType.MESH
VMEM_LIMIT = 60 * 1024 * 1024
f32 = jnp.float32
bf16 = jnp.bfloat16


def greet(peers):
    barrier = pltpu.get_barrier_semaphore()
    for peer in peers:
        pl.semaphore_signal(barrier, inc=1, device_id=peer, device_id_type=MESH)
    pl.semaphore_wait(barrier, len(peers))


def line_and_pair(n):
    me = lax.axis_index("sp")
    lines = n // 2
    outer, inner = me // 2, lax.rem(me, 2)
    partner = {"sp": outer * 2 + 1 - inner}

    def line_peer(d):
        return {"sp": lax.rem(outer + d, lines) * 2 + inner}

    return me, lines, outer, inner, partner, line_peer


def project_kernel(n, count, *refs):
    tokens_ref, gain_ref, rate_ref = refs[:3]
    weights = refs[3 : 3 + count]
    (
        v_ref,
        gate_ref,
        ql_ref,
        ll_ref,
        fq_ref,
        fk_ref,
        bq_ref,
        bk_ref,
        log_ref,
        f_state_ref,
        b_state_ref,
    ) = refs[3 + count : 14 + count]
    rest = refs[14 + count :]
    x_ref, x_recv = rest[0], rest[1]
    w_recv = rest[2 : 2 + count]
    p_send = rest[2 + count : 2 + 2 * count]
    p_recv = rest[2 + 2 * count : 2 + 3 * count]
    own = rest[2 + 3 * count : 2 + 4 * count]
    xs, xr, ws, wr, ps, pr = rest[2 + 4 * count :]
    groups = n // 4
    me = lax.axis_index("sp")
    group, place = me // 4, lax.rem(me, 4)
    low, inner = place // 2, lax.rem(place, 2)
    places = (
        place,
        (1 - low) * 2 + inner,
        low * 2 + 1 - inner,
        (1 - low) * 2 + 1 - inner,
    )
    beside = {"sp": group * 4 + places[1]}
    partner = {"sp": group * 4 + places[2]}

    def far_peer(d):
        return {"sp": lax.rem(group + d, groups) * 4 + place}

    greet([beside, partner] + [far_peer(d) for d in range(1, groups)])

    def w_copy(c, k):
        return pltpu.make_async_remote_copy(
            src_ref=w_recv[c].at[0] if k == 2 else weights[c],
            dst_ref=w_recv[c].at[k],
            send_sem=ws.at[c, k],
            recv_sem=wr.at[c, k],
            device_id=beside if k == 0 else partner,
            device_id_type=MESH,
        )

    def x_copy(d):
        return pltpu.make_async_remote_copy(
            src_ref=x_ref.at[lax.rem(group + d, groups)],
            dst_ref=x_recv.at[d],
            send_sem=xs.at[d],
            recv_sem=xr.at[d],
            device_id=far_peer(d),
            device_id_type=MESH,
        )

    def p_copy(c, d):
        return pltpu.make_async_remote_copy(
            src_ref=p_send[c].at[d],
            dst_ref=p_recv[c].at[d],
            send_sem=ps.at[c, d],
            recv_sem=pr.at[c, d],
            device_id=far_peer(d),
            device_id_type=MESH,
        )

    w_copy(0, 0).start()
    for c in range(3):
        w_copy(c, 1).start()
    wide = tokens_ref[...].astype(f32)
    scale = lax.rsqrt(jnp.mean(wide * wide, axis=-1, keepdims=True) + norm_eps)
    normed = (wide * scale * gain_ref[...]).astype(bf16)
    rows, depth = x_ref.shape[2:]
    for g in range(groups):
        for k in range(4):
            first = (g * 4 + k) * depth
            x_ref[g, k] = normed[:, first : first + depth]
    for d in range(1, groups):
        x_copy(d).start()
    for c in range(1, count):
        w_copy(c, 0).start()
    for c in range(count):
        w_copy(c, 0).wait_recv()
        w_copy(c, 2).start()
        if c + 3 < count:
            w_copy(c + 3, 1).start()
    def finished(c):
        def add(d, total):
            p_copy(c, d).wait_recv()
            return total + p_recv[c][d].astype(f32)

        return lax.fori_loop(1, groups, add, own[c][...]).astype(bf16)

    def recurrence():
        value = finished(0)
        v_ref[...] = value
        row = lax.broadcasted_iota(jnp.int32, (rows, rows), 0)
        col = lax.broadcasted_iota(jnp.int32, (rows, rows), 1)

        def direction(c, mask, last):
            rate = rate_ref[c - 1 : c, :] / (rows * n)
            key = rate * jax.nn.sigmoid(-finished(c).astype(f32))
            total = jnp.dot(
                jnp.where(mask, 1.0, 0.0),
                jnp.log1p(-key),
                precision=lax.Precision.HIGHEST,
                preferred_element_type=f32,
            )
            full = total[last : last + 1, :]
            key = (key * jnp.exp(-total)).astype(bf16)
            state = jnp.concatenate(
                [
                    lax.dot_general(
                        value[:, h * VAL_DIM : (h + 1) * VAL_DIM],
                        key[:, h * KEY_DIM : (h + 1) * KEY_DIM],
                        (((0,), (0,)), ((), ())),
                        preferred_element_type=f32,
                    )
                    for h in range(value.shape[1] // VAL_DIM)
                ],
                axis=1,
            )
            log_ref[c - 1 : c, :] = full
            return key, total, (state * jnp.exp(full)).astype(bf16)

        fk_ref[...], f_total, f_state_ref[...] = direction(1, row >= col, rows - 1)
        bk_ref[...], b_total, b_state_ref[...] = direction(2, row <= col, 0)
        query = finished(3).astype(f32)
        fq_ref[...] = (query * jnp.exp(f_total)).astype(bf16)
        bq_ref[...] = (query * jnp.exp(b_total)).astype(bf16)

    for c in range(count):
        w_copy(c, 1).wait_recv()
        w_copy(c, 2).wait_recv()

        def part(x):
            total = jnp.dot(x(places[0]), weights[c][...], preferred_element_type=f32)
            for k in range(3):
                total += jnp.dot(x(places[k + 1]), w_recv[c][k], preferred_element_type=f32)
            return total

        @pl.loop(1, groups)
        def _(d):
            if c == 0:
                x_copy(d).wait_recv()
            back = groups - d
            p_send[c][back] = part(lambda k: x_recv[d, k]).astype(bf16)
            p_copy(c, back).start()

        own[c][...] = part(lambda k: x_ref[group, k])
        if c == count - 2:
            recurrence()
    gate_ref[...] = finished(4)
    ql_ref[...] = finished(5)
    ll_ref[...] = finished(6)
    for d in range(1, groups):
        x_copy(d).wait_send()
    for c in range(count):
        for k in range(3):
            w_copy(c, k).wait_send()

        @pl.loop(1, groups)
        def _(d):
            p_copy(c, d).wait_send()


def project_all(n, tokens, gain, rates, weights):
    groups = n // 4
    rows, depth = tokens.shape[0], weights[0].shape[0]
    count = len(weights)
    widths = [w.shape[1] for w in weights]
    width = widths[0]
    wide = jax.ShapeDtypeStruct((rows, width), bf16)
    state = jax.ShapeDtypeStruct((VAL_DIM, width), bf16)
    vmem = pl.BlockSpec(memory_space=pltpu.VMEM)
    return pl.pallas_call(
        functools.partial(project_kernel, n, count),
        out_shape=[jax.ShapeDtypeStruct((rows, widths[c]), bf16) for c in (0, 4, 5, 6)]
        + [wide] * 4
        + [jax.ShapeDtypeStruct((2, width), f32), state, state],
        in_specs=[vmem] * (3 + count),
        out_specs=[vmem] * 11,
        scratch_shapes=[pltpu.VMEM((groups, 4, rows, depth), bf16)] * 2
        + [pltpu.VMEM((3, depth, c), bf16) for c in widths]
        + [pltpu.VMEM((groups, rows, c), bf16) for c in widths]
        + [pltpu.VMEM((groups, rows, c), bf16) for c in widths]
        + [pltpu.VMEM((rows, c), f32) for c in widths]
        + [
            pltpu.SemaphoreType.DMA((groups,)),
            pltpu.SemaphoreType.DMA((groups,)),
            pltpu.SemaphoreType.DMA((count, 3)),
            pltpu.SemaphoreType.DMA((count, 3)),
            pltpu.SemaphoreType.DMA((count, groups)),
            pltpu.SemaphoreType.DMA((count, groups)),
        ],
        compiler_params=pltpu.CompilerParams(
            collective_id=0, has_side_effects=True, vmem_limit_bytes=VMEM_LIMIT
        ),
    )(tokens, gain, rates, *weights)


def heads_peer(n, d):
    return {"tp": lax.rem(lax.axis_index("tp") + d, n)}


def mixer_kernel(n, heads_n, *refs):
    count = 5
    query_in, pair_in, ins = refs[0], refs[1], refs[2 : 2 + count]
    (
        fq_ref,
        fk_ref,
        bq_ref,
        bk_ref,
        v_ref,
        gate_ref,
        chain_gain_ref,
        query_latent_gain_ref,
        latent_gain_ref,
        query_up_ref,
        latent_up_ref,
        query_gain_ref,
        key_gain_ref,
        mixer_gain_ref,
        query_tail_ref,
        key_tail_ref,
        cos_ref,
        sin_ref,
        pick_key_ref,
        swap_key_ref,
        pick_plain_ref,
        pick_query_ref,
        swap_query_ref,
        out_ref,
    ) = refs[2 + count : 26 + count]
    rest = refs[26 + count :]
    query_out, pair_out, outs = rest[0], rest[1], rest[2 : 2 + count]
    numer, denom, send, recv, keep, s1, r1, s2, r2, hs1, hr1, hs2, hr2, ss, rs = rest[2 + count :]
    me, lines, outer, inner, partner, line_peer = line_and_pair(n)
    head = lax.axis_index("tp")
    head_lines = heads_n // 2
    head_outer, head_inner = head // 2, lax.rem(head, 2)
    head_partner = {"tp": head_outer * 2 + 1 - head_inner}

    def head_peer(d):
        return {"tp": lax.rem(head_outer + d, head_lines) * 2 + head_inner}

    greet(
        [partner]
        + [line_peer(d) for d in range(1, lines)]
        + [heads_peer(heads_n, d) for d in range(1, heads_n)]
    )
    src = (pair_in,) + tuple(ins)

    def slot(k, at):
        return pair_out.at[head, at] if k == 0 else outs[k - 1].at[at]

    def along(k, d):
        return pltpu.make_async_remote_copy(
            src_ref=src[k],
            dst_ref=slot(k, me),
            send_sem=s1.at[k, d],
            recv_sem=r1.at[k, d],
            device_id=line_peer(d),
            device_id_type=MESH,
        )

    def across(k, d):
        at = lax.rem(outer - d + lines, lines) * 2 + inner
        return pltpu.make_async_remote_copy(
            src_ref=src[k] if isinstance(d, int) and d == 0 else slot(k, at),
            dst_ref=slot(k, at),
            send_sem=s2.at[k, d],
            recv_sem=r2.at[k, d],
            device_id=partner,
            device_id_type=MESH,
        )

    def local(k):
        return pltpu.make_async_copy(src[k], slot(k, me), keep.at[k])

    def head_along(j, d):
        return pltpu.make_async_remote_copy(
            src_ref=query_in if j == 0 else pair_out.at[head],
            dst_ref=query_out.at[head] if j == 0 else pair_out.at[head],
            send_sem=hs1.at[j, d],
            recv_sem=hr1.at[j, d],
            device_id=head_peer(d),
            device_id_type=MESH,
        )

    def head_across(j, d):
        at = lax.rem(head_outer - d + head_lines, head_lines) * 2 + head_inner
        own = isinstance(d, int) and d == 0
        out = query_out if j == 0 else pair_out
        return pltpu.make_async_remote_copy(
            src_ref=query_in if j == 0 and own else out.at[at],
            dst_ref=out.at[at],
            send_sem=hs2.at[j, d],
            recv_sem=hr2.at[j, d],
            device_id=head_partner,
            device_id_type=MESH,
        )

    query_local = pltpu.make_async_copy(query_in, query_out.at[head], keep.at[1 + count])

    def needed(k, there):
        if k == 2:
            return there
        if k == 3:
            return jnp.logical_not(there)
        return None

    def maybe(condition, act):
        if condition is None:
            act()
        else:
            pl.when(condition)(act)

    def on_line(k, sending, act):
        @pl.loop(1, lines)
        def _(d):
            there = outer + d < lines if sending else outer >= d
            maybe(needed(k, there), lambda: act(d))

    for k in range(1 + count):
        on_line(k, True, lambda d: along(k, d).start())
        across(k, 0).start()
        local(k).start()
        if k == 0:
            for d in range(1, head_lines):
                head_along(0, d).start()
            head_across(0, 0).start()
            query_local.start()

    def pass_on(k):
        def act(d):
            along(k, d).wait_recv()
            across(k, d).start()

        on_line(k, False, act)

    pass_on(0)
    for d in range(1, head_lines):
        head_along(0, d).wait_recv()
        head_across(0, d).start()
    local(0).wait()
    across(0, 0).wait_recv()
    on_line(0, False, lambda d: across(0, d).wait_recv())
    for d in range(1, head_lines):
        head_along(1, d).start()
    head_across(1, 0).start()
    for k in range(1, count - 1):
        pass_on(k)

    rows, width = v_ref.shape
    chain_heads = width // KEY_DIM

    def lanes(h, size):
        return slice(h * size, (h + 1) * size)

    def against(a, b):
        return lax.dot_general(a, b, (((1,), (1,)), ((), ())), preferred_element_type=f32)

    row = lax.broadcasted_iota(jnp.int32, (rows, rows), 0)
    col = lax.broadcasted_iota(jnp.int32, (rows, rows), 1)
    within = []
    for h in range(chain_heads):
        at = lanes(h, KEY_DIM)
        both = jnp.where(row >= col, against(fq_ref[:, at], fk_ref[:, at]), 0.0) + jnp.where(
            row <= col, against(bq_ref[:, at], bk_ref[:, at]), 0.0
        )
        within.append(
            jnp.dot(both.astype(bf16), v_ref[:, lanes(h, VAL_DIM)], preferred_element_type=f32)
        )

    for d in range(1, head_lines):
        head_along(1, d).wait_recv()
        head_across(1, d).start()
    for k in (1, 2, 3):
        local(k).wait()
        across(k, 0).wait_recv()
        on_line(k, False, lambda d: across(k, d).wait_recv())

    log_ref, f_ref, b_ref = outs[0], outs[1], outs[2]

    def forward(i, state):
        return state * jnp.exp(log_ref[i, 0:1, :]) + f_ref[i].astype(f32)

    def backward(i, state):
        at = n - 1 - i
        return state * jnp.exp(log_ref[at, 1:2, :]) + b_ref[at].astype(f32)

    nothing = jnp.zeros(f_ref.shape[1:], f32)
    f_in = lax.fori_loop(0, me, forward, nothing).astype(bf16)
    b_in = lax.fori_loop(0, n - 1 - me, backward, nothing).astype(bf16)

    def normed(values, size):
        return lax.rsqrt(jnp.sum(values * values, axis=-1, keepdims=True) / size + norm_eps)

    chain_parts = []
    for h in range(chain_heads):
        at = lanes(h, KEY_DIM)
        total = (
            within[h] + against(fq_ref[:, at], f_in[:, at]) + against(bq_ref[:, at], b_in[:, at])
        )
        gate = gate_ref[:, lanes(h, VAL_DIM)].astype(f32)
        scaled = total * normed(total, VAL_DIM) * chain_gain_ref[:, lanes(h, VAL_DIM)]
        chain_parts.append((scaled * (gate * jax.nn.sigmoid(gate))).astype(bf16))
    chain_mixed = jnp.concatenate(chain_parts, axis=1)
    pass_on(4)

    query_local.wait()
    for j in range(head_lines):
        head_across(0, j).wait_recv()
    raws = [query_out[t].astype(f32) for t in range(heads_n)]
    q_cols = raws[0].shape[1]
    square = sum(jnp.sum(r * r, axis=-1, keepdims=True) for r in raws)
    scale = lax.rsqrt(square / (heads_n * q_cols) + norm_eps)
    attend_q = sum(
        jnp.dot(
            (raws[t] * scale * query_latent_gain_ref[t]).astype(bf16),
            query_up_ref[lanes(t, q_cols), :],
            preferred_element_type=f32,
        )
        for t in range(heads_n)
    ).astype(bf16)
    heads = pick_plain_ref.shape[0]
    query_cos = cos_ref[me] * query_tail_ref[0:1, :]
    query_sin = sin_ref[me] * query_tail_ref[1:2, :]
    q_plain, q_turned = [], []
    for h in range(heads):
        plain = jnp.dot(attend_q, pick_plain_ref[h], preferred_element_type=f32)
        tail = jnp.dot(attend_q, pick_query_ref[h], preferred_element_type=f32)
        swapped = jnp.dot(attend_q, swap_query_ref[h], preferred_element_type=f32)
        square = jnp.sum(plain * plain, axis=-1, keepdims=True) + jnp.sum(
            tail * tail, axis=-1, keepdims=True
        )
        scale = lax.rsqrt(square / ATT_QK + norm_eps)
        q_plain.append((plain * scale * query_gain_ref[...]).astype(bf16))
        q_turned.append(
            ((tail * query_cos + swapped * query_sin) * scale).astype(bf16)
        )

    for d in range(head_lines):
        head_across(1, d).wait_recv()
    numer[...] = jnp.zeros_like(numer)
    denom[...] = jnp.zeros_like(denom)
    l_cols = latent_up_ref.shape[0] // heads_n

    def attend(at, carry):
        pieces = [pair_out[t, at] for t in range(heads_n)]
        wide = [p[:, :l_cols].astype(f32) for p in pieces]
        square = sum(jnp.sum(w * w, axis=-1, keepdims=True) for w in wide)
        scale = lax.rsqrt(square / (heads_n * l_cols) + norm_eps)
        latent = jnp.concatenate(
            [
                (wide[t] * scale * latent_gain_ref[:, lanes(t, l_cols)]).astype(bf16)
                for t in range(heads_n)
            ],
            axis=1,
        )
        pairs = jnp.dot(latent, latent_up_ref[...], preferred_element_type=f32).astype(bf16)
        tail = sum(
            jnp.dot(pieces[t], pick_key_ref[t], preferred_element_type=f32)
            for t in range(heads_n)
        )
        swapped = sum(
            jnp.dot(pieces[t], swap_key_ref[t], preferred_element_type=f32)
            for t in range(heads_n)
        )
        tail_square = jnp.sum(tail * tail, axis=-1, keepdims=True)
        turned = (tail * key_tail_ref[0:1, :]) * cos_ref[at] + (
            swapped * key_tail_ref[1:2, :]
        ) * sin_ref[at]
        for h in range(heads):
            start = h * (NOPE_DIM + VHEAD_DIM)
            plain = pairs[:, start : start + NOPE_DIM].astype(f32)
            value = pairs[:, start + NOPE_DIM : start + NOPE_DIM + VHEAD_DIM]
            square = jnp.sum(plain * plain, axis=-1, keepdims=True) + tail_square
            scale = lax.rsqrt(square / ATT_QK + norm_eps)
            score = against(
                q_plain[h], (plain * scale * key_gain_ref[...]).astype(bf16)
            ) + against(q_turned[h], (turned * scale).astype(bf16))
            weight = jnp.exp(score * ATT_QK ** (-0.5))
            numer[h] += jnp.dot(weight.astype(bf16), value, preferred_element_type=f32)
            denom[h] += jnp.sum(weight, axis=-1, keepdims=True)
        return carry

    lax.fori_loop(0, n // 2, attend, 0)
    pass_on(5)
    lax.fori_loop(n // 2, n, attend, 0)
    attend_parts = []
    for h in range(heads):
        total = numer[h] / denom[h]
        gain = mixer_gain_ref[:, lanes(h, VHEAD_DIM)]
        attend_parts.append((total * normed(total, VHEAD_DIM) * gain).astype(bf16))
    attend_mixed = jnp.concatenate(attend_parts, axis=1)

    for k in (4, 5):
        local(k).wait()
        across(k, 0).wait_recv()
        on_line(k, False, lambda d: across(k, d).wait_recv())
    wc_ref, wa_ref = outs[3], outs[4]
    col_n = wc_ref.shape[2]
    part_rows = rows // heads_n
    for i in range(n):
        product = jnp.dot(chain_mixed, wc_ref[i], preferred_element_type=f32) + jnp.dot(
            attend_mixed, wa_ref[i], preferred_element_type=f32
        )
        for t in range(heads_n):
            send[t, :, lanes(i, col_n)] = product[lanes(t, part_rows)].astype(bf16)

    def sum_copy(d):
        return pltpu.make_async_remote_copy(
            src_ref=send.at[lax.rem(head + d, heads_n)],
            dst_ref=recv.at[d],
            send_sem=ss.at[d],
            recv_sem=rs.at[d],
            device_id=heads_peer(heads_n, d),
            device_id_type=MESH,
        )

    for d in range(1, heads_n):
        sum_copy(d).start()
    total = send[head].astype(f32)
    for d in range(1, heads_n):
        sum_copy(d).wait_recv()
        total = total + recv[d].astype(f32)
    out_ref[...] = total

    for d in range(1, heads_n):
        sum_copy(d).wait_send()
    for k in range(1 + count):
        across(k, 0).wait_send()
        on_line(k, True, lambda d: along(k, d).wait_send())
        on_line(k, False, lambda d: across(k, d).wait_send())
    for j in range(2):
        head_across(j, 0).wait_send()
        for d in range(1, head_lines):
            head_along(j, d).wait_send()
            head_across(j, d).wait_send()


def mix_all(n, heads_n, query, pair, blocks, others, heads):
    lines, head_lines = n // 2, heads_n // 2
    count = len(blocks)
    rows = query.shape[0]
    out_cols = n * blocks[-1].shape[1]
    vmem = pl.BlockSpec(memory_space=pltpu.VMEM)
    return pl.pallas_call(
        functools.partial(mixer_kernel, n, heads_n),
        out_shape=jax.ShapeDtypeStruct((rows // heads_n, out_cols), f32),
        in_specs=[vmem] * (2 + count + len(others)),
        out_specs=vmem,
        scratch_shapes=[
            pltpu.VMEM((heads_n,) + query.shape, query.dtype),
            pltpu.VMEM((heads_n, n) + pair.shape, pair.dtype),
        ]
        + [pltpu.VMEM((n,) + b.shape, b.dtype) for b in blocks]
        + [
            pltpu.VMEM((heads, rows, VHEAD_DIM), f32),
            pltpu.VMEM((heads, rows, 1), f32),
            pltpu.VMEM((heads_n, rows // heads_n, out_cols), bf16),
            pltpu.VMEM((heads_n, rows // heads_n, out_cols), bf16),
            pltpu.SemaphoreType.DMA((2 + count,)),
        ]
        + [pltpu.SemaphoreType.DMA((1 + count, lines))] * 4
        + [pltpu.SemaphoreType.DMA((2, head_lines))] * 4
        + [pltpu.SemaphoreType.DMA((heads_n,))] * 2,
        compiler_params=pltpu.CompilerParams(
            collective_id=1, has_side_effects=True, vmem_limit_bytes=VMEM_LIMIT
        ),
    )(query, pair, *blocks, *others)


def on_device(
    tokens,
    input_gain,
    chain_query,
    forward_gate,
    backward_gate,
    chain_value,
    output_gate,
    forget_rate,
    chain_gain,
    query_down,
    latent_down,
    rotary_down,
    query_latent_gain,
    latent_gain,
    query_up,
    latent_up,
    query_head_gain,
    key_head_gain,
    mixer_gain,
    chain_out,
    attend_out,
):
    n_sp, n_tp = lax.axis_size("sp"), lax.axis_size("tp")
    sp, tp = lax.axis_index("sp"), lax.axis_index("tp")
    rows, depth = tokens.shape[0], chain_query.shape[0]
    seq_len = rows * n_sp
    q_cols = query_down.shape[1] // n_tp
    l_cols = latent_down.shape[1] // n_tp
    r_cols = ROPE_DIM // n_tp
    q_down = lax.dynamic_slice_in_dim(query_down, tp * q_cols, q_cols, 1)
    l_down = jnp.concatenate(
        [
            lax.dynamic_slice_in_dim(latent_down, tp * l_cols, l_cols, 1),
            lax.dynamic_slice(rotary_down, (sp * depth, tp * r_cols), (depth, r_cols)),
        ],
        axis=1,
    )
    (v_rows, gate_logit, raw_q, raw_l, f_q, f_k, b_q, b_k, logs, f_state, b_state) = project_all(
        n_sp,
        tokens,
        input_gain[None],
        forget_rate,
        (chain_value, forward_gate, backward_gate, chain_query, output_gate, q_down, l_down),
    )

    heads = query_up.shape[1] // ATT_QK
    half = ROPE_DIM // 2
    inverse = rope_theta ** (-np.arange(0, ROPE_DIM, 2).astype(np.float32) / ROPE_DIM)
    angles = np.arange(seq_len, dtype=np.float32)[:, None] * inverse.astype(np.float32)
    cosine, sine = (
        jnp.asarray(np.tile(turn(angles), (1, 2)).reshape(n_sp, rows, ROPE_DIM), f32)
        for turn in (np.cos, np.sin)
    )

    def tails(gain):
        tail = gain[NOPE_DIM:]
        return jnp.stack([tail, jnp.roll(tail, half)])

    swap = np.zeros((ROPE_DIM, ROPE_DIM), np.float32)
    for j in range(half):
        swap[half + j, j] = -1.0
        swap[j, half + j] = 1.0
    pick_key = np.zeros((n_tp, l_cols + r_cols, ROPE_DIM), np.float32)
    for t in range(n_tp):
        for j in range(r_cols):
            pick_key[t, l_cols + j, t * r_cols + j] = 1.0
    pick_plain = np.zeros((heads, heads * ATT_QK, NOPE_DIM), np.float32)
    pick_query = np.zeros((heads, heads * ATT_QK, ROPE_DIM), np.float32)
    for h in range(heads):
        for j in range(NOPE_DIM):
            pick_plain[h, h * ATT_QK + j, j] = 1.0
        for j in range(ROPE_DIM):
            pick_query[h, h * ATT_QK + NOPE_DIM + j, j] = 1.0
    picks = [
        jnp.asarray(p, bf16)
        for p in (pick_key, pick_key @ swap, pick_plain, pick_query, pick_query @ swap)
    ]
    return mix_all(
        n_sp,
        n_tp,
        raw_q,
        raw_l,
        (logs, f_state, b_state, chain_out, attend_out),
        (
            f_q,
            f_k,
            b_q,
            b_k,
            v_rows,
            gate_logit,
            chain_gain[None],
            query_latent_gain.reshape(n_tp, 1, q_cols),
            latent_gain[None],
            query_up,
            latent_up,
            query_head_gain[None, :NOPE_DIM],
            key_head_gain[None, :NOPE_DIM],
            mixer_gain[None],
            tails(query_head_gain),
            tails(key_head_gain),
            cosine,
            sine,
            *picks,
        ),
        heads,
    )


def solution(mesh):
    placed = (
        P("sp", None),
        P(),
        P("sp", "tp"),
        P("sp", "tp"),
        P("sp", "tp"),
        P("sp", "tp"),
        P("sp", "tp"),
        P(None, "tp"),
        P("tp"),
        P("sp", None),
        P("sp", None),
        P(),
        P(),
        P(),
        P(None, "tp"),
        P(None, "tp"),
        P(),
        P(),
        P("tp"),
        P("tp", "sp"),
        P("tp", "sp"),
    )
    return jax.shard_map(
        on_device, mesh=mesh, in_specs=placed, out_specs=P(("sp", "tp"), None), check_vma=False
    )
```
